32 devices in a mesh: sp: 8 (over z, y), tp: 4 (over x, core).
Axes of the slice: x: 2, y: 2, z: 4, core: 2. Of those that a mesh axis runs over, the one named last changes fastest.
Arguments:
- cotangent: bfloat16 [1536, 4096], P('sp'), may hold values from -6 to 6
- moe_input: bfloat16 [1536, 4096], P('sp'), may hold values from -6 to 6
- routes: int32 [1536, 2], P('sp'), may hold values from 0 to 7, all different within a row; in each aligned block of 192 rows (0 to 191, 192 to 383, ...) at most 96 rows name the same one
- route_weight: float32 [1536, 2], P('sp'), may hold values from 0.3 to 1.7
- conv_input: bfloat16 [1536, 2048], P('sp', 'tp'), may hold values from -6 to 6
- input_gate: bfloat16 [1536, 2048], P('sp', 'tp'), may hold values from -6 to 6
- output_gate: bfloat16 [1536, 2048], P('sp', 'tp'), may hold values from -6 to 6
- conv_output: bfloat16 [1536, 2048], P('sp', 'tp'), may hold values from -6 to 6
- taps: float32 [3, 2048], P(None, 'tp'), may hold values from -3 to 3
- w_out: bfloat16 [4096, 2048], P(None, 'tp'), may hold values from -0.125 to 0.125
- w_gate: bfloat16 [8, 4096, 1024], P('sp', None, 'tp'), may hold values from -0.09375 to 0.09375
- w_up: bfloat16 [8, 4096, 1024], P('sp', None, 'tp'), may hold values from -0.09375 to 0.09375
- w_down: bfloat16 [8, 1024, 4096], P('sp', 'tp'), may hold values from -0.1875 to 0.1875
Outputs:
- grad_w_gate: bfloat16 [8, 4096, 1024], P('sp', None, 'tp')
- grad_w_up: bfloat16 [8, 4096, 1024], P('sp', None, 'tp')
- grad_w_down: bfloat16 [8, 1024, 4096], P('sp', 'tp')
- grad_w_out: float32 [4096, 2048], P('sp', 'tp')
- grad_conv_input: bfloat16 [1536, 2048], P('sp', 'tp')
- grad_input_gate: bfloat16 [1536, 2048], P('sp', 'tp')
- grad_output_gate: bfloat16 [1536, 2048], P('sp', 'tp')
The draws below stay inside these ranges and needn't reach their ends.
Inputs may be any that keep to these rules, and one draw needn't show every extreme that they name: `routes`: each row names 2 different experts. Among the rows of one index of sp no expert is named by more than 96 rows, and in every draw some expert is named by exactly 96 rows of some index.
All inputs are finite; a program needn't handle non-finite values.
Results may differ from the reference program's by a relative error of at most 0.0065.
Values may be sent and summed in bfloat16 or wider, within the bound.
A program may use at most 192 MiB of HBM per device.

```python
import math
import jax
import jax.numpy as jnp
import numpy as np
from jax import lax

D = 4096
FF = 1024
B_WIDTH = 2048
TAPS = 3
TOP = 2
TOK_DEV = 192
TOKENS = 1536
EXPERTS = 8
CAP = 96
N_SP = 8


def with_spikes(result, stream_key, source, target, blocks, factor):
    def block_of(axis_at):
        return (jnp.arange(result.shape[axis_at]) // (result.shape[axis_at] // blocks)).reshape((-1,) + (1,) * (result.ndim - 1 - axis_at))

    near = jax.random.permutation(stream_key, blocks)[block_of(target)]
    second = (block_of(target) + blocks // 2) % blocks
    return jnp.where((block_of(source) == near) | (block_of(source) == second), factor * result, result)


def block_scale(rng, dims, pieces, low, high):
    def one(position, parts):
        heights = jax.random.uniform(jax.random.fold_in(jax.random.fold_in(rng, 6), position), (parts,), jnp.float32, low / len(pieces), high / len(pieces))
        return jnp.repeat(jnp.exp(heights), dims[position] // parts).reshape((-1,) + (1,) * (len(dims) - position - 1))

    gain = one(*pieces[0])
    for cut in pieces[1:]:
        gain = gain * one(*cut)
    return gain


def shared_out(key, own, number, rows, number_of, top, limit, lean):
    sequence = jax.random.permutation(key, number_of)
    packed, usual = load_shares(number_of, rows * top, limit, lean, True), load_shares(number_of, rows * top, limit, lean, False)
    places = jnp.arange(number_of)

    def named(lengths, rotation):
        used = int((lengths > 0).sum())
        fixed = max(1, used // 4)
        moved = fixed + (places - fixed + rotation * (used - fixed)) % max(1, number_of - fixed)
        return jnp.zeros((number_of,), jnp.int32).at[sequence[jnp.where(places < fixed, places, moved)]].set(jnp.asarray(lengths, jnp.int32))

    lengths = jnp.where(number % 4 == 0, named(packed, number // 4), named(usual, number - number // 4 - 1))
    mixed = jax.random.permutation(jax.random.fold_in(own, 3), number_of)
    giver, taker = mixed[0:number_of // 2 * 2:2], mixed[1:number_of // 2 * 2:2]
    room = jnp.minimum(lengths[giver] - 1, limit - lengths[taker]) // 2
    room = jnp.where((giver == sequence[0]) | (taker == sequence[0]) | (lengths[taker] == 0), 0, jnp.maximum(room, 0))
    moved = jax.random.randint(jax.random.fold_in(own, 4), (number_of // 2,), 0, 1 << 20) % (room + 1)
    lengths = lengths.at[giver].add(-moved).at[taker].add(moved)
    items = jnp.searchsorted(jnp.cumsum(lengths), jnp.arange(rows * top), side="right").astype(jnp.int32)
    listing = items.reshape(top, rows).T
    listing = listing[jax.random.permutation(jax.random.fold_in(own, 1), rows)]
    rotation = jax.random.randint(jax.random.fold_in(own, 2), (rows, 1), 0, top)
    return jnp.take_along_axis(listing, (jnp.arange(top)[None, :] + rotation) % top, axis=1)


def load_shares(count, total, bound, skew, full):
    portions = [(1 << 20) // math.isqrt(standing ** skew) + 1 for standing in range(1, count + 1)]
    largest = bound if full else min(bound, max(-(-total // count), total * portions[0] // sum(portions)))
    least = 1 if total - largest >= count - 1 else 0
    holding, surplus = [largest] + [least] * (count - 1), total - largest - least * (count - 1)
    while surplus > 0:
        candidates = [i for i in range(1, count) if holding[i] < largest] or [i for i in range(1, count) if holding[i] < bound]
        whole, left = sum([portions[i] for i in candidates]), surplus
        for i in candidates:
            more = min(bound - holding[i], max(1, left * portions[i] // whole), surplus)
            holding[i] = holding[i] + more
            surplus = surplus - more
    return np.array(holding)


def noise(rng, extent, spread, most, pieces=(), kind=jnp.bfloat16):
    array = jax.random.normal(rng, extent, jnp.float32) * spread
    if len(pieces) > 0:
        array = block_scale(rng, extent, pieces, -0.22, 0.18) * array
    return jnp.clip(array, min=-most, max=most).astype(kind)


def noise_with(rng, shape, spread, reach, shards, heavy, held_as=jnp.bfloat16):
    drawn = spread * jax.random.normal(rng, shape, jnp.float32)
    if shards:
        drawn = drawn * block_scale(rng, shape, shards, -0.22, 0.18)
    return jnp.clip(with_spikes(drawn, jax.random.fold_in(rng, 3), *heavy), -reach, reach).astype(held_as)


def setup_inputs(seed: int = 0) -> dict:
    key_list = jax.random.split(jax.random.key(seed), 14)
    cotangent = noise_with(key_list[0], (TOKENS, D), 1.0, 6.0, ((0, 8),), (0, 1, 8, 2.0))
    moe_input = noise(key_list[1], (TOKENS, D), 1.0, 6.0, ((0, 8),))
    routes_keys = jax.random.split(jax.random.fold_in(key_list[2], 1), TOKENS // TOK_DEV)
    routes_turns = jax.random.permutation(jax.random.fold_in(key_list[2], 3), TOKENS // TOK_DEV)
    routes = jax.vmap(lambda own, number: shared_out(jax.random.fold_in(key_list[2], 2), own, number, TOK_DEV, EXPERTS, TOP, CAP, 2))(routes_keys, routes_turns).reshape((TOKENS, TOP))
    route_weight = jnp.clip(0.3 + 1.40000004 * jax.random.uniform(key_list[3], (TOKENS, TOP), jnp.float32) ** block_scale(key_list[3], (TOKENS, TOP), ((0, 8),), -0.2, 0.2), 0.3, 1.7)
    conv_input = noise(key_list[4], (TOKENS, B_WIDTH), 1.0, 6.0, ((0, 8), (1, 4)))
    input_gate = noise(key_list[5], (TOKENS, B_WIDTH), 1.0, 6.0, ((0, 8), (1, 4)))
    output_gate = noise(key_list[6], (TOKENS, B_WIDTH), 1.0, 6.0, ((0, 8), (1, 4)))
    conv_output = noise(key_list[7], (TOKENS, B_WIDTH), 1.0, 6.0, ((0, 8), (1, 4)))
    taps = noise(key_list[8], (TAPS, B_WIDTH), 0.6, 3.0, ((1, 4),), jnp.float32)
    w_out = noise(key_list[9], (D, B_WIDTH), B_WIDTH ** -0.5, 0.125, ((1, 4),))
    w_gate = noise(key_list[10], (EXPERTS, D, FF), D ** -0.5, 0.09375, ((0, 8), (2, 4)))
    w_up = noise(key_list[11], (EXPERTS, D, FF), D ** -0.5, 0.09375, ((0, 8), (2, 4)))
    w_down = noise(key_list[12], (EXPERTS, FF, D), FF ** -0.5, 0.1875, ((0, 8), (1, 4)))
    return {"cotangent": cotangent, "moe_input": moe_input, "routes": routes, "route_weight": route_weight, "conv_input": conv_input, "input_gate": input_gate, "output_gate": output_gate, "conv_output": conv_output, "taps": taps, "w_out": w_out, "w_gate": w_gate, "w_up": w_up, "w_down": w_down}


def silu_parts(gate_proj):
    sigmoid_gate = jax.nn.sigmoid(gate_proj)
    activated = gate_proj * sigmoid_gate
    slope = sigmoid_gate * (1.0 + gate_proj * (1.0 - sigmoid_gate))
    return activated, slope


def expert_backward(scaled_rows, input_rows, gate_weight, up_weight, down_weight):
    gate_proj = jnp.dot(input_rows, gate_weight, preferred_element_type=jnp.float32)
    up_proj = jnp.dot(input_rows, up_weight, preferred_element_type=jnp.float32)
    activated, slope = silu_parts(gate_proj)
    hidden = (activated * up_proj).astype(jnp.bfloat16)
    grad_down = lax.dot_general(hidden, scaled_rows, (((0,), (0,)), ((), ())), preferred_element_type=jnp.float32)
    grad_hidden = lax.dot_general(scaled_rows, down_weight, (((1,), (1,)), ((), ())), preferred_element_type=jnp.float32)
    grad_gate = (grad_hidden * up_proj * slope).astype(jnp.bfloat16)
    grad_up = (grad_hidden * activated).astype(jnp.bfloat16)
    gate_wgrad = lax.dot_general(input_rows, grad_gate, (((0,), (0,)), ((), ())), preferred_element_type=jnp.float32)
    up_wgrad = lax.dot_general(input_rows, grad_up, (((0,), (0,)), ((), ())), preferred_element_type=jnp.float32)
    row_part = lax.dot_general(grad_gate, gate_weight, (((1,), (1,)), ((), ())), preferred_element_type=jnp.float32)
    row_part = row_part + lax.dot_general(grad_up, up_weight, (((1,), (1,)), ((), ())), preferred_element_type=jnp.float32)
    return gate_wgrad, up_wgrad, grad_down, row_part


def reference(cotangent, moe_input, routes, route_weight, conv_input, input_gate, output_gate, conv_output, taps, w_out, w_gate, w_up, w_down):
    tok_total = cotangent.shape[0]
    model_width = cotangent.shape[1]
    row_count = N_SP * CAP
    zero_row = jnp.zeros((1, model_width), jnp.bfloat16)
    padded_cot = jnp.concatenate([cotangent, zero_row], axis=0)
    padded_inp = jnp.concatenate([moe_input, zero_row], axis=0)

    def per_expert(expert):
        matched = routes == expert
        expert_weight = jnp.sum(jnp.where(matched, route_weight, jnp.zeros_like(route_weight)), axis=1)
        expert_weight = jnp.concatenate([expert_weight, jnp.zeros((1,), route_weight.dtype)])
        row_index = jnp.nonzero(jnp.any(matched, axis=1), size=row_count, fill_value=tok_total)[0].astype(jnp.int32)
        scaled_rows = (expert_weight[row_index][:, None] * padded_cot[row_index].astype(jnp.float32)).astype(jnp.bfloat16)
        input_rows = padded_inp[row_index]
        gate_wgrad, up_wgrad, grad_down, row_part = expert_backward(scaled_rows, input_rows, w_gate[expert], w_up[expert], w_down[expert])
        return (gate_wgrad.astype(jnp.bfloat16), up_wgrad.astype(jnp.bfloat16), grad_down.astype(jnp.bfloat16),
                row_part.astype(jnp.bfloat16), row_index)

    gate_grads, up_grads, down_grads, route_grads, row_indices = lax.map(per_expert, jnp.arange(EXPERTS, dtype=jnp.int32))
    accumulated = jnp.zeros((tok_total + 1, model_width), jnp.float32)
    accumulated = accumulated.at[row_indices.reshape(-1)].add(route_grads.reshape(-1, model_width).astype(jnp.float32))
    resid_grad = (cotangent.astype(jnp.float32) + accumulated[:tok_total]).astype(jnp.bfloat16)

    mixed = (output_gate.astype(jnp.float32) * conv_output.astype(jnp.float32)).astype(jnp.bfloat16)
    grad_w_out = jnp.dot(resid_grad.T, mixed, preferred_element_type=jnp.float32)
    grad_mixed = jnp.dot(resid_grad, w_out, preferred_element_type=jnp.float32)
    grad_output_gate = (grad_mixed * conv_output.astype(jnp.float32)).astype(jnp.bfloat16)
    grad_conv = grad_mixed * output_gate.astype(jnp.float32)
    extended = jnp.concatenate([grad_conv, jnp.zeros((2, grad_conv.shape[1]), jnp.float32)], axis=0)
    grad_g = taps[2] * extended[:tok_total] + taps[1] * extended[1:tok_total + 1] + taps[0] * extended[2:]
    grad_conv_input = (grad_g * input_gate.astype(jnp.float32)).astype(jnp.bfloat16)
    grad_input_gate = (grad_g * conv_input.astype(jnp.float32)).astype(jnp.bfloat16)
    return (gate_grads, up_grads, down_grads, grad_w_out, grad_conv_input, grad_input_gate, grad_output_gate)
```

```python
import functools

import jax
import jax.numpy as jnp
from jax import lax
from jax.experimental import pallas as pl
from jax.experimental.pallas import tpu as pltpu
from jax.sharding import PartitionSpec as P

MESH = pl.DeviceIdType.MESH
NN = (((1,), (0,)), ((), ()))
NT = (((1,), (1,)), ((), ()))
TN = (((0,), (0,)), ((), ()))


def dot(a, b, dims=NN):
    return lax.dot_general(a, b, dims, preferred_element_type=jnp.float32)


def each(low, high, step):
    def body(i, carry):
        step(i)
        return carry

    lax.fori_loop(low, high, body, 0)


def spot():
    s, t = lax.axis_index("sp"), lax.axis_index("tp")
    return s, t, lax.div(t, 2), lax.rem(t, 2)


def greet(S, TH):
    s, t, th, tl = spot()
    barrier = pltpu.get_barrier_semaphore()

    def hello(device):
        pl.semaphore_signal(barrier, inc=1, device_id=device, device_id_type=MESH)

    each(1, S, lambda k: hello((lax.rem(s + k, S), t)))
    hello((s, 2 * th + 1 - tl))
    for j in range(1, TH):
        hello((s, 2 * lax.rem(th + j, TH) + tl))
    pl.semaphore_wait(barrier, S - 1 + TH)


def expert_kernel(
    S, T, inp, cot, placed, slot_w, wg_h, wu_h, wd_h,
    back, gwg_h, gwu_h, gwd_h,
    rows, stage, wgu, wd, proj, hid, ggu, part, matebuf, xsend, xrecv, rstage, gout, gdown,
    wsem, gsem, ds, dr, m1s, m1r, xs, xr, m2s, m2r, r1s, r1r, r2s, r2r, rts, rtr,
):
    TH = T // 2
    cap, Q = rows.shape[3], rows.shape[4]
    D = T * Q
    H = wd.shape[0]
    piece = Q // S
    group = D // S
    s, t, th, tl = spot()
    mate = 2 * th + 1 - tl
    source = (inp, cot)

    def other(j):
        return lax.rem(th + j, TH)

    def behind(j):
        return lax.rem(th - j + TH, TH)

    def src_of(k):
        return lax.rem(s - k + S, S)

    weights = [
        pltpu.make_async_copy(wg_h, wgu.at[:, pl.ds(0, H)], wsem.at[0]),
        pltpu.make_async_copy(wu_h, wgu.at[:, pl.ds(H, H)], wsem.at[1]),
        pltpu.make_async_copy(wd_h, wd, wsem.at[2]),
    ]
    for copy in weights:
        copy.start()
    greet(S, TH)

    def remote(src, dst, send, recv, device):
        return pltpu.make_async_remote_copy(
            src_ref=src, dst_ref=dst, send_sem=send, recv_sem=recv, device_id=device, device_id_type=MESH
        )

    def direct(a, k):
        return remote(stage.at[a, k], rows.at[a, s, t], ds.at[a, k], dr.at[a, k], (lax.rem(s + k, S), t))

    def to_mate(a, k):
        block = rows.at[a, src_of(k), t]
        return remote(block, block, m1s.at[a, k], m1r.at[a, k], (s, mate))

    def across(a, j, k):
        block = rows.at[a, src_of(k), t]
        return remote(block, block, xs.at[a, j, k], xr.at[a, j, k], (s, 2 * other(j) + tl))

    def on_to_mate(a, j, k):
        block = rows.at[a, src_of(k), 2 * behind(j) + tl]
        return remote(block, block, m2s.at[a, j, k], m2r.at[a, j, k], (s, mate))

    def pick(a, e, columns):
        picked = dot(placed[e], source[a][:, columns])
        if a == 1:
            picked = picked * slot_w[e]
        return picked.astype(jnp.bfloat16)

    def send(a, k):
        stage[a, k] = pick(a, lax.rem(s + k, S), pl.ds(pl.multiple_of(t * Q, Q), Q))
        direct(a, k).start()

    def own(a):
        for q in range(T):
            rows[a, s, q] = pick(a, s, pl.ds(q * Q, Q))

    def forward(a, k):
        direct(a, k).wait_recv()
        for j in range(1, TH):
            across(a, j, k).start()
        to_mate(a, k).start()

    def forward_on(a, k):
        for j in range(1, TH):
            across(a, j, k).wait_recv()
            on_to_mate(a, j, k).start()

    def complete(a, k):
        to_mate(a, k).wait_recv()
        for j in range(1, TH):
            on_to_mate(a, j, k).wait_recv()

    def project(k):
        b = src_of(k)
        total = dot(rows[0, b, 0], wgu[pl.ds(0, Q), :])
        for q in range(1, T):
            total = total + dot(rows[0, b, q], wgu[pl.ds(q * Q, Q), :])
        proj[b] = total

    def half(k):
        return remote(
            part.at[lax.rem(k, 2), 1 - tl], matebuf.at[k], r1s.at[k], r1r.at[k], (s, mate)
        )

    def chip_sum(j, k):
        return remote(xsend.at[j, k], xrecv.at[j, k], r2s.at[j, k], r2r.at[j, k], (s, 2 * other(j) + tl))

    def give_back(k):
        return remote(rstage.at[k], back.at[s], rts.at[k], rtr.at[k], (src_of(k), t))

    def gradients(k):
        b = src_of(k)
        grad_hidden = dot(rows[1, b, 0], wd[:, pl.ds(0, Q)], NT)
        for q in range(1, T):
            grad_hidden = grad_hidden + dot(rows[1, b, q], wd[:, pl.ds(q * Q, Q)], NT)
        gate, up = proj[b][:, :H], proj[b][:, H:]
        sig = jax.nn.sigmoid(gate)
        act = gate * sig
        slope = sig * (1.0 + gate * (1.0 - sig))
        hid[b] = (act * up).astype(jnp.bfloat16)
        ggu[b, :, pl.ds(0, H)] = (grad_hidden * up * slope).astype(jnp.bfloat16)
        ggu[b, :, pl.ds(H, H)] = (grad_hidden * act).astype(jnp.bfloat16)

        @pl.when(k >= 2)
        def _():
            half(k - 2).wait_send()

        slot = lax.rem(k, 2)
        grads = ggu[b]
        for g in range(S):
            some = dot(grads, wgu[pl.ds(g * group, group), :], NT)
            for q in range(T):
                part[slot, q % 2, q // 2, :, pl.ds(g * piece, piece)] = some[:, q * piece : (q + 1) * piece]
        half(k).start()

    def reduce_chip(k):
        half(k).wait_recv()
        slot = lax.rem(k, 2)
        for j in range(1, TH):
            o = other(j)
            xsend[j, k] = (part[slot, tl, o] + matebuf[k, o]).astype(jnp.bfloat16)
            chip_sum(j, k).start()
        matebuf[k, th] = part[slot, tl, th] + matebuf[k, th]

    def reduce_all(k):
        total = matebuf[k, th]
        for j in range(1, TH):
            chip_sum(j, k).wait_recv()
            total = total + xrecv[j, k].astype(jnp.float32)
        rstage[k] = total.astype(jnp.bfloat16)

        @pl.when(k >= 1)
        def _():
            give_back(k).start()

    keep = pltpu.make_async_copy(rstage.at[0], back.at[s], rts.at[0])

    each(1, S, lambda k: send(0, k))
    own(0)
    each(1, S, lambda k: send(1, k))
    own(1)
    for copy in weights:
        copy.wait()
    project(0)

    def first(i):
        @pl.when(i < S)
        def _():
            forward(0, i)

        @pl.when((i >= 2) & (i < S + 1))
        def _():
            forward_on(0, i - 1)

        @pl.when(i >= 3)
        def _():
            complete(0, i - 2)
            project(i - 2)

    each(1, S + 2, first)
    gradients(0)

    def second(i):
        @pl.when(i < S)
        def _():
            forward(1, i)

        @pl.when((i >= 2) & (i < S + 1))
        def _():
            forward_on(1, i - 1)

        @pl.when((i >= 3) & (i < S + 3))
        def _():
            reduce_chip(i - 3)

        @pl.when((i >= 3) & (i < S + 2))
        def _():
            complete(1, i - 2)
            gradients(i - 2)

        @pl.when(i >= 4)
        def _():
            reduce_all(i - 4)

    each(1, S + 4, second)
    keep.start()

    tile = min(512, Q)
    per = Q // tile

    def weight_grads(i):
        q, c = lax.div(i, per), pl.multiple_of(lax.rem(i, per) * tile, tile)
        x = rows[0, :, q, :, pl.ds(c, tile)].reshape(S * cap, tile)
        start = pl.multiple_of(q * Q + c, tile)
        gout[pl.ds(start, tile), :] = dot(x, ggu[...].reshape(S * cap, 2 * H), TN).astype(jnp.bfloat16)
        d = rows[1, :, q, :, pl.ds(c, tile)].reshape(S * cap, tile)
        gdown[:, pl.ds(start, tile)] = dot(hid[...].reshape(S * cap, H), d, TN).astype(jnp.bfloat16)

    each(0, T * per, weight_grads)
    results = [
        pltpu.make_async_copy(gout.at[:, pl.ds(0, H)], gwg_h, gsem.at[0]),
        pltpu.make_async_copy(gout.at[:, pl.ds(H, H)], gwu_h, gsem.at[1]),
        pltpu.make_async_copy(gdown, gwd_h, gsem.at[2]),
    ]
    for copy in results:
        copy.start()

    half(S - 2).wait_send()
    half(S - 1).wait_send()

    def finish(k):
        for a in range(2):
            direct(a, k).wait_send()
            to_mate(a, k).wait_send()
            for j in range(1, TH):
                across(a, j, k).wait_send()
                on_to_mate(a, j, k).wait_send()
        give_back(k).wait_send()
        give_back(k).wait_recv()

    each(1, S, finish)

    def finish_sums(k):
        for j in range(1, TH):
            chip_sum(j, k).wait_send()

    each(0, S, finish_sums)
    keep.wait()
    for copy in results:
        copy.wait()


def expert_exchange(S, T, cap, inp, cot, placed, slot_w, w_gate, w_up, w_down):
    tok, D = inp.shape
    H = w_down.shape[0]
    TH, Q = T // 2, D // T
    bf, f32 = jnp.bfloat16, jnp.float32
    dma = pltpu.SemaphoreType.DMA
    vmem = pl.BlockSpec(memory_space=pltpu.VMEM)
    hbm = pl.BlockSpec(memory_space=pl.ANY)
    rows = S * cap
    return pl.pallas_call(
        functools.partial(expert_kernel, S, T),
        name="expert_exchange",
        out_shape=(
            jax.ShapeDtypeStruct((S, cap, Q), bf),
            jax.ShapeDtypeStruct((D, H), bf),
            jax.ShapeDtypeStruct((D, H), bf),
            jax.ShapeDtypeStruct((H, D), bf),
        ),
        in_specs=[vmem] * 4 + [hbm] * 3,
        out_specs=(hbm,) * 4,
        scratch_shapes=[
            pltpu.VMEM((2, S, T, cap, Q), bf),
            pltpu.VMEM((2, S, cap, Q), bf),
            pltpu.VMEM((D, 2 * H), bf),
            pltpu.VMEM((H, D), bf),
            pltpu.VMEM((S, cap, 2 * H), f32),
            pltpu.VMEM((S, cap, H), bf),
            pltpu.VMEM((S, cap, 2 * H), bf),
            pltpu.VMEM((2, 2, TH, cap, Q), f32),
            pltpu.VMEM((S, TH, cap, Q), f32),
            pltpu.VMEM((TH, S, cap, Q), bf),
            pltpu.VMEM((TH, S, cap, Q), bf),
            pltpu.VMEM((S, cap, Q), bf),
            pltpu.VMEM((D, 2 * H), bf),
            pltpu.VMEM((H, D), bf),
            dma((3,)), dma((3,)),
            dma((2, S)), dma((2, S)),
            dma((2, S)), dma((2, S)),
            dma((2, TH, S)), dma((2, TH, S)),
            dma((2, TH, S)), dma((2, TH, S)),
            dma((S,)), dma((S,)),
            dma((TH, S)), dma((TH, S)),
            dma((S,)), dma((S,)),
        ],
        cost_estimate=pl.CostEstimate(
            flops=16 * rows * D * H, bytes_accessed=8 * rows * D + 24 * D * H, transcendentals=rows * H
        ),
        compiler_params=pltpu.CompilerParams(
            collective_id=0, has_side_effects=True, vmem_limit_bytes=67_043_328
        ),
    )(inp, cot, placed, slot_w, w_gate, w_up, w_down)


def slot_masks(routes, route_weight, experts, capacity):
    tok_rows = routes.shape[0]
    names = jnp.arange(experts, dtype=jnp.int32)
    hits = routes[None, :, :] == names[:, None, None]
    chosen = jnp.any(hits, axis=2)
    weight = jnp.sum(jnp.where(hits, route_weight[None], 0.0), axis=2)
    order = jnp.arange(tok_rows, dtype=jnp.int32)
    before = (order[:, None] < order[None, :]).astype(jnp.bfloat16)
    rank = jnp.dot(chosen.astype(jnp.bfloat16), before, preferred_element_type=jnp.float32)
    rank = jnp.where(chosen, rank.astype(jnp.int32), -1)
    slots = jnp.arange(capacity, dtype=jnp.int32)
    placed = rank[:, None, :] == slots[None, :, None]
    slot_weight = jnp.sum(jnp.where(placed, weight[:, None, :], 0.0), axis=2, keepdims=True)
    return placed.astype(jnp.bfloat16), slot_weight


def from_behind(value, axis, steps):
    count = lax.axis_size(axis)
    leading, last = (max(0, -steps), min(count, count - steps))
    return lax.ppermute(value, axis, [(source, source + steps) for source in range(leading, last)])


def per_device(
    cotangent, moe_input, routes, route_weight, conv_input, input_gate, output_gate, conv_output,
    taps, w_out, w_gate, w_up, w_down,
):
    experts = lax.axis_size("sp")
    tp_size = lax.axis_size("tp")
    tok_rows, top_k = routes.shape
    model_width = cotangent.shape[1]
    capacity = -(-max(2, 2 * tok_rows * top_k // experts) // 16) * 16
    part_width = model_width // tp_size
    piece = part_width // experts
    tp_index = lax.axis_index("tp")
    placed, slot_weight = slot_masks(routes, route_weight, experts, capacity)
    returned, gate_wgrad, up_wgrad, grad_down = expert_exchange(
        experts, tp_size, capacity, moe_input, cotangent, placed, slot_weight, w_gate[0], w_up[0], w_down[0]
    )
    mixed = (output_gate.astype(jnp.float32) * conv_output.astype(jnp.float32)).astype(jnp.bfloat16)

    def over_sp(value):
        return lax.all_to_all(value, "sp", split_axis=0, concat_axis=0, tiled=True)

    out_turned = w_out.reshape(experts, tp_size, piece, -1).swapaxes(0, 1).reshape(model_width, -1)
    cot_share = cotangent.reshape(tok_rows, experts, tp_size, piece)
    cot_share = lax.dynamic_index_in_dim(cot_share, tp_index, 2, keepdims=False)
    cot_share = cot_share.reshape(tok_rows, part_width)
    mixed_all = over_sp(jnp.broadcast_to(mixed[None], (experts,) + mixed.shape))
    mixed_all = mixed_all.reshape(experts * tok_rows, -1)
    route_sum = cot_share.astype(jnp.float32) + lax.dot_general(
        placed.reshape(experts * capacity, tok_rows),
        returned.reshape(experts * capacity, part_width),
        (((0,), (0,)), ((), ())),
        preferred_element_type=jnp.float32,
    )
    resid_part = route_sum.astype(jnp.bfloat16)
    resid_grad = lax.all_gather(resid_part, "tp", axis=1, tiled=True)
    own = over_sp(jnp.swapaxes(resid_part.reshape(tok_rows, experts, piece), 0, 1))
    resid_cols = lax.all_gather(own, "tp", axis=2, tiled=True)
    resid_cols = resid_cols.reshape(experts * tok_rows, model_width // experts)
    grad_w_out = lax.dot_general(
        resid_cols, mixed_all, (((0,), (0,)), ((), ())), preferred_element_type=jnp.float32
    )
    grad_mixed = jnp.dot(resid_grad, out_turned, preferred_element_type=jnp.float32)
    grad_output_gate = (grad_mixed * conv_output.astype(jnp.float32)).astype(jnp.bfloat16)
    grad_conv = grad_mixed * output_gate.astype(jnp.float32)
    following = from_behind(grad_conv[:2], "sp", -1)
    extended = jnp.concatenate([grad_conv, following], axis=0)
    grad_g = (
        taps[2] * extended[:tok_rows]
        + taps[1] * extended[1 : tok_rows + 1]
        + taps[0] * extended[2:]
    )
    grad_conv_input = (grad_g * input_gate.astype(jnp.float32)).astype(jnp.bfloat16)
    grad_input_gate = (grad_g * conv_input.astype(jnp.float32)).astype(jnp.bfloat16)
    return (
        gate_wgrad[None], up_wgrad[None], grad_down[None], grad_w_out,
        grad_conv_input, grad_input_gate, grad_output_gate,
    )


def solution(mesh):
    return jax.shard_map(
        per_device,
        mesh=mesh,
        in_specs=(
            P("sp", None), P("sp", None), P("sp", None), P("sp", None),
            P("sp", "tp"), P("sp", "tp"), P("sp", "tp"), P("sp", "tp"),
            P(None, "tp"), P(None, "tp"),
            P("sp", None, "tp"), P("sp", None, "tp"), P("sp", "tp", None),
        ),
        out_specs=(
            P("sp", None, "tp"), P("sp", None, "tp"), P("sp", "tp", None),
            P("sp", "tp"), P("sp", "tp"), P("sp", "tp"), P("sp", "tp"),
        ),
        check_vma=False,
    )
```

```python
import functools

import jax
import jax.numpy as jnp
from jax import lax
from jax.experimental import pallas as pl
from jax.experimental.pallas import tpu as pltpu
from jax.sharding import PartitionSpec as P

NEAR = 2
MESH = pl.DeviceIdType.MESH
NN = (((1,), (0,)), ((), ()))
NT = (((1,), (1,)), ((), ()))
TN = (((0,), (0,)), ((), ()))


def dot(a, b, dims=NN):
    return lax.dot_general(a, b, dims, preferred_element_type=jnp.float32)


def each(low, high, step):
    def body(i, carry):
        step(i)
        return carry

    lax.fori_loop(low, high, body, 0)


def spot():
    s, t = lax.axis_index("sp"), lax.axis_index("tp")
    return s, t, lax.div(t, 2), lax.rem(t, 2)


def flip(S, a, b):
    total, weight = 0, 1
    while weight < S:
        p, q = lax.rem(lax.div(a, weight), 2), lax.rem(lax.div(b, weight), 2)
        total, weight = total + (p + q - 2 * p * q) * weight, 2 * weight
    return total


def partner(S, s, i):
    if S < 4:
        return i
    high, low = lax.div(s, S // 2), lax.rem(lax.div(s, S // 4), 2)
    inner = high + low - 2 * high * low
    turned = S // 2 + lax.rem(i - S // 2 + inner * (S // 4) + S, S // 2)
    return jnp.where(i >= S // 2, turned, i)


def remote(src, dst, send, recv, device):
    return pltpu.make_async_remote_copy(
        src_ref=src, dst_ref=dst, send_sem=send, recv_sem=recv, device_id=device, device_id_type=MESH
    )


def greet(S, TH):
    s, t, th, tl = spot()
    barrier = pltpu.get_barrier_semaphore()

    def hello(device):
        pl.semaphore_signal(barrier, inc=1, device_id=device, device_id_type=MESH)

    each(1, S, lambda k: hello((lax.rem(s + k, S), t)))
    hello((s, 2 * th + 1 - tl))
    for j in range(1, TH):
        hello((s, 2 * lax.rem(th + j, TH) + tl))
    pl.semaphore_wait(barrier, S - 1 + TH)


def expert_kernel(
    S, T, inp, cot, placed, slot_w, out_gate, conv_out, wg_h, wu_h, wd_h,
    back, mix_all, gwg_h, gwu_h, gwd_h,
    mix, rows, stage, wgu, wd, proj, hid, ggu, part, matebuf, total_part, near, xsend, xrecv, rstage, gout, gdown,
    wsem, gsem, ds, dr, m1s, m1r, xs, xr, m2s, m2r, r1s, r1r, r2s, r2r, rts, rtr, us, ur, vs, vr, ys, yr,
):
    TH = T // 2
    cap, Q = rows.shape[3], rows.shape[4]
    D = T * Q
    H = wd.shape[0]
    piece = Q // S
    group = D // S
    s, t, th, tl = spot()
    mate = 2 * th + 1 - tl
    source = (inp, cot)

    def other(j):
        return lax.rem(th + j, TH)

    def behind(j):
        return lax.rem(th - j + TH, TH)

    def src_of(k):
        return flip(S, s, k)

    def at(i):
        return partner(S, s, i)

    weights = [
        pltpu.make_async_copy(wg_h, wgu.at[:, pl.ds(0, H)], wsem.at[0]),
        pltpu.make_async_copy(wu_h, wgu.at[:, pl.ds(H, H)], wsem.at[1]),
        pltpu.make_async_copy(wd_h, wd, wsem.at[2]),
    ]
    for copy in weights:
        copy.start()
    greet(S, TH)

    def direct(a, k):
        return remote(stage.at[a, k], rows.at[a, s, t], ds.at[a, k], dr.at[a, k], (src_of(k), t))

    def direct_too(a, j, k):
        q = 2 * other(j) + tl
        return remote(near.at[a, j, k], rows.at[a, s, q], xs.at[a, j, k], xr.at[a, TH - j, k], (src_of(k), t))

    def to_mate(a, k):
        block = rows.at[a, src_of(k), t]
        return remote(block, block, m1s.at[a, k], m1r.at[a, k], (s, mate))

    def across(a, j, k):
        block = rows.at[a, src_of(k), t]
        return remote(block, block, xs.at[a, j, k], xr.at[a, j, k], (s, 2 * other(j) + tl))

    def on_to_mate(a, j, k):
        block = rows.at[a, src_of(k), 2 * behind(j) + tl]
        return remote(block, block, m2s.at[a, j, k], m2r.at[a, j, k], (s, mate))

    def pick(a, e, columns):
        picked = dot(placed[e], source[a][:, columns])
        if a == 1:
            picked = picked * slot_w[e]
        return picked.astype(jnp.bfloat16)

    def send(a, k):
        stage[a, k] = pick(a, src_of(k), pl.ds(pl.multiple_of(t * Q, Q), Q))
        direct(a, k).start()

        @pl.when(k < NEAR)
        def _():
            for j in range(1, TH):
                near[a, j, k] = pick(a, src_of(k), pl.ds(pl.multiple_of((2 * other(j) + tl) * Q, Q), Q))
                direct_too(a, j, k).start()

    def own(a):
        for q in range(T):
            rows[a, s, q] = pick(a, s, pl.ds(q * Q, Q))

    def forward(a, k):
        direct(a, k).wait_recv()

        @pl.when(k >= NEAR)
        def _():
            for j in range(1, TH):
                across(a, j, k).start()

        to_mate(a, k).start()

    def forward_on(a, k):
        for j in range(1, TH):
            across(a, j, k).wait_recv()
            on_to_mate(a, j, k).start()

    def complete(a, k):
        to_mate(a, k).wait_recv()
        for j in range(1, TH):
            on_to_mate(a, j, k).wait_recv()

    def project(k):
        b = src_of(k)
        total = dot(rows[0, b, 0], wgu[pl.ds(0, Q), :])
        for q in range(1, T):
            total = total + dot(rows[0, b, q], wgu[pl.ds(q * Q, Q), :])
        proj[b] = total

    def half(n):
        return remote(part.at[lax.rem(n, 2), 1 - tl], matebuf.at[n], r1s.at[n], r1r.at[n], (s, mate))

    def chip_sum(j, k):
        return remote(xsend.at[j, k], xrecv.at[j, k], r2s.at[j, k], r2r.at[j, k], (s, 2 * other(j) + tl))

    def give_back(k):
        return remote(rstage.at[k], back.at[s], rts.at[k], rtr.at[k], (src_of(k), t))

    def gradients(n, k):
        b = src_of(k)
        grad_hidden = dot(rows[1, b, 0], wd[:, pl.ds(0, Q)], NT)
        for q in range(1, T):
            grad_hidden = grad_hidden + dot(rows[1, b, q], wd[:, pl.ds(q * Q, Q)], NT)
        gate, up = proj[b][:, :H], proj[b][:, H:]
        sig = jax.nn.sigmoid(gate)
        act = gate * sig
        slope = sig * (1.0 + gate * (1.0 - sig))
        hid[b] = (act * up).astype(jnp.bfloat16)
        ggu[b, :, pl.ds(0, H)] = (grad_hidden * up * slope).astype(jnp.bfloat16)
        ggu[b, :, pl.ds(H, H)] = (grad_hidden * act).astype(jnp.bfloat16)

        @pl.when(n >= 2)
        def _():
            half(n - 2).wait_send()

        slot = lax.rem(n, 2)
        grads = ggu[b]
        for g in range(S):
            some = dot(grads, wgu[pl.ds(g * group, group), :], NT)
            for q in range(T):
                part[slot, q % 2, q // 2, :, pl.ds(g * piece, piece)] = some[:, q * piece : (q + 1) * piece]
        half(n).start()

    def reduce_chip(n, k):
        half(n).wait_recv()
        slot = lax.rem(n, 2)
        for j in range(1, TH):
            o = other(j)
            xsend[j, k] = (part[slot, tl, o] + matebuf[n, o]).astype(jnp.bfloat16)
            chip_sum(j, k).start()
        total_part[slot] = part[slot, tl, th] + matebuf[n, th]

    def reduce_all(n, k):
        total = total_part[lax.rem(n, 2)]
        for j in range(1, TH):
            chip_sum(j, k).wait_recv()
            total = total + xrecv[j, k].astype(jnp.float32)
        rstage[k] = total.astype(jnp.bfloat16)

        @pl.when(k >= 1)
        def _():
            give_back(k).start()

    SH = S // 2
    sh, sl = lax.div(s, 2), lax.rem(s, 2)

    def block(h):
        return mix_all.at[2 * h + sl]

    def rise(j):
        return remote(mix if j == 0 else block(sh - j), block(sh - j), us.at[j], ur.at[j + 1], (s + 2, t))

    def sink(j):
        return remote(mix if j == 0 else block(sh + j), block(sh + j), vs.at[j], vr.at[j + 1], (s - 2, t))

    def side(h, value=None):
        return remote(block(h) if value is None else value, block(h), ys.at[h], yr.at[h], (2 * sh + 1 - sl, t))

    def mix_step(j):
        if j == 0:
            side(sh, mix).start()

            @pl.when(sh < SH - 1)
            def _():
                rise(0).start()

            @pl.when(sh > 0)
            def _():
                sink(0).start()

            return

        @pl.when(sh >= j)
        def _():
            remote(block(sh - j), block(sh - j), us.at[j], ur.at[j], (s, mate)).wait_recv()

            @pl.when(sh < SH - 1)
            def _():
                rise(j).start()

            side(sh - j).start()

        @pl.when(sh + j < SH)
        def _():
            remote(block(sh + j), block(sh + j), vs.at[j], vr.at[j], (s, mate)).wait_recv()

            @pl.when(sh > 0)
            def _():
                sink(j).start()

            side(sh + j).start()

    def mix_finish():
        keep_mix.wait()
        for j in range(SH - 1):

            @pl.when((sh >= j) & (sh < SH - 1))
            def _():
                rise(j).wait_send()

            @pl.when((sh + j < SH) & (sh > 0))
            def _():
                sink(j).wait_send()

        def one(h):
            side(h).wait_send()
            side(h).wait_recv()

        each(0, SH, one)

    keep_mix = pltpu.make_async_copy(mix, mix_all.at[s], gsem.at[3])
    keep = pltpu.make_async_copy(rstage.at[0], back.at[s], rts.at[0])

    each(1, S, lambda i: send(0, at(i)))
    own(0)
    mix[...] = (out_gate[...].astype(jnp.float32) * conv_out[...].astype(jnp.float32)).astype(jnp.bfloat16)
    own(1)
    for copy in weights:
        copy.wait()
    project(0)

    def first(i):
        @pl.when(i < S)
        def _():
            forward(0, at(i))
            send(1, at(i))

        @pl.when((i >= 2) & (i < S + 1))
        def _():
            forward_on(0, at(i - 1))

        @pl.when(i >= 3)
        def _():
            complete(0, at(i - 2))
            project(at(i - 2))

    each(1, S + 2, first)
    mix_step(0)
    gradients(0, 0)

    def second(i):
        @pl.when(i < S)
        def _():
            forward(1, at(i))

        @pl.when((i >= 2) & (i < S + 1))
        def _():
            forward_on(1, at(i - 1))

        @pl.when((i >= 3) & (i < S + 3))
        def _():
            reduce_chip(i - 3, at(i - 3))

        @pl.when((i >= 3) & (i < S + 2))
        def _():
            complete(1, at(i - 2))
            gradients(i - 2, at(i - 2))

        @pl.when(i >= 4)
        def _():
            reduce_all(i - 4, at(i - 4))

        for j in range(1, SH):

            @pl.when(i == 2 * j)
            def _():
                mix_step(j)

    each(1, S + 4, second)
    keep.start()
    keep_mix.start()

    tile = min(512, Q)
    per = Q // tile

    def weight_grads(i):
        q, c = lax.div(i, per), pl.multiple_of(lax.rem(i, per) * tile, tile)
        x = rows[0, :, q, :, pl.ds(c, tile)].reshape(S * cap, tile)
        start = pl.multiple_of(q * Q + c, tile)
        gout[pl.ds(start, tile), :] = dot(x, ggu[...].reshape(S * cap, 2 * H), TN).astype(jnp.bfloat16)
        d = rows[1, :, q, :, pl.ds(c, tile)].reshape(S * cap, tile)
        gdown[:, pl.ds(start, tile)] = dot(hid[...].reshape(S * cap, H), d, TN).astype(jnp.bfloat16)

    each(0, T * per, weight_grads)
    results = [
        pltpu.make_async_copy(gout.at[:, pl.ds(0, H)], gwg_h, gsem.at[0]),
        pltpu.make_async_copy(gout.at[:, pl.ds(H, H)], gwu_h, gsem.at[1]),
        pltpu.make_async_copy(gdown, gwd_h, gsem.at[2]),
    ]
    for copy in results:
        copy.start()

    half(S - 2).wait_send()
    half(S - 1).wait_send()

    def finish(k):
        for a in range(2):
            direct(a, k).wait_send()
            to_mate(a, k).wait_send()
            for j in range(1, TH):
                across(a, j, k).wait_send()
                on_to_mate(a, j, k).wait_send()
        give_back(k).wait_send()
        give_back(k).wait_recv()

    each(1, S, finish)

    def finish_sums(k):
        for j in range(1, TH):
            chip_sum(j, k).wait_send()

    each(0, S, finish_sums)
    keep.wait()
    mix_finish()
    for copy in results:
        copy.wait()


def mixer_kernel(
    S, T, placed, cot, out_gate, conv_out, in_gate, conv_in, taps, back_h, mix_h, w_out_h,
    gwo, gci, gig, gog,
    back, mix, w_out, total, res, colst, cols, conv, after,
    lsem, ds, dr, m1s, m1r, xs, xr, m2s, m2r, bs, br,
):
    TH = T // 2
    cap, Q = back.shape[1], back.shape[2]
    tok = cot.shape[0]
    piece, group = Q // S, T * Q // S
    s, t, th, tl = spot()
    mate = 2 * th + 1 - tl
    local = [
        pltpu.make_async_copy(src, dst, lsem.at[n])
        for n, (src, dst) in enumerate(((back_h, back), (mix_h, mix), (w_out_h, w_out)))
    ]
    for copy in local:
        copy.start()
    greet(S, TH)

    def other(j):
        return lax.rem(th + j, TH)

    def behind(j):
        return lax.rem(th - j + TH, TH)

    def at(i):
        return partner(S, s, i)

    def direct(k):
        peer = flip(S, s, k)
        return remote(colst.at[peer], cols.at[s, t], ds.at[k], dr.at[k], (peer, t))

    def block(k, q):
        return cols.at[flip(S, s, k), q] if k is not None else res.at[q]

    def to_mate(k):
        n = S if k is None else k
        return remote(block(k, t), block(k, t), m1s.at[n], m1r.at[n], (s, mate))

    def across(j, k):
        n = S if k is None else k
        return remote(block(k, t), block(k, t), xs.at[j, n], xr.at[j, n], (s, 2 * other(j) + tl))

    def on_to_mate(j, k):
        n = S if k is None else k
        q = 2 * behind(j) + tl
        return remote(block(k, q), block(k, q), m2s.at[j, n], m2r.at[j, n], (s, mate))

    def forward(k):
        for j in range(1, TH):
            across(j, k).start()
        to_mate(k).start()

    def forward_on(k):
        for j in range(1, TH):
            across(j, k).wait_recv()
            on_to_mate(j, k).start()

    def complete(k):
        to_mate(k).wait_recv()
        for j in range(1, TH):
            on_to_mate(j, k).wait_recv()

    def sent(k):
        to_mate(k).wait_send()
        for j in range(1, TH):
            across(j, k).wait_send()
            on_to_mate(j, k).wait_send()

    local[0].wait()
    total[...] = dot(placed[...].reshape(S * cap, tok), back[...].reshape(S * cap, Q), TN)
    for q in range(T):

        @pl.when(t == q)
        def _():
            for g in range(S):
                columns = pl.ds(g * piece, piece)
                mine = cot[:, pl.ds(g * group + q * piece, piece)].astype(jnp.float32)
                value = (mine + total[:, columns]).astype(jnp.bfloat16)
                res[q, :, columns] = value
                colst[g] = value

    forward(None)
    each(1, S, lambda i: direct(at(i)).start())
    cols[s, t] = colst[s]
    forward(0)

    def arrive(i):
        direct(at(i)).wait_recv()
        forward(at(i))

    local[2].wait()
    forward_on(None)
    each(1, S, arrive)
    complete(None)
    grad_mixed = jnp.zeros((tok, w_out.shape[1]), jnp.float32)
    for g in range(S):
        some = jnp.concatenate([res[q, :, pl.ds(g * piece, piece)] for q in range(T)], axis=1)
        grad_mixed = grad_mixed + dot(some, w_out[pl.ds(g * group, group), :])
    gog[...] = (grad_mixed * conv_out[...].astype(jnp.float32)).astype(jnp.bfloat16)
    conv[pl.ds(0, tok), :] = grad_mixed * out_gate[...].astype(jnp.float32)

    def edge(target):
        return remote(conv.at[pl.ds(0, 8), :], after, bs.at[0], br.at[0], (target, t))

    @pl.when(s > 0)
    def _():
        edge(s - 1).start()

    local[1].wait()

    def take(k):
        complete(k)
        b = flip(S, s, k)
        columns = jnp.concatenate([cols[b, q] for q in range(T)], axis=1)
        gwo[...] += dot(columns, mix[b], TN)

    gwo[...] = jnp.zeros_like(gwo)
    forward_on(0)

    def step(i):
        @pl.when(i < S)
        def _():
            forward_on(at(i))

        take(at(i - 1))

    each(1, S + 1, step)

    @pl.when(s < S - 1)
    def _():
        edge(0).wait_recv()
        conv[pl.ds(tok, 8), :] = after[...]

    @pl.when(s == S - 1)
    def _():
        conv[pl.ds(tok, 8), :] = jnp.zeros_like(after)

    grad_g = (
        taps[2:3, :] * conv[pl.ds(0, tok), :]
        + taps[1:2, :] * conv[pl.ds(1, tok), :]
        + taps[0:1, :] * conv[pl.ds(2, tok), :]
    )
    gci[...] = (grad_g * in_gate[...].astype(jnp.float32)).astype(jnp.bfloat16)
    gig[...] = (grad_g * conv_in[...].astype(jnp.float32)).astype(jnp.bfloat16)

    @pl.when(s > 0)
    def _():
        edge(s - 1).wait_send()

    sent(None)
    each(0, S, sent)
    each(1, S, lambda k: direct(k).wait_send())


def expert_exchange(S, T, cap, inp, cot, placed, slot_w, out_gate, conv_out, w_gate, w_up, w_down):
    tok, D = inp.shape
    H = w_down.shape[0]
    TH, Q, SH = T // 2, D // T, S // 2
    bf, f32 = jnp.bfloat16, jnp.float32
    dma = pltpu.SemaphoreType.DMA
    vmem = pl.BlockSpec(memory_space=pltpu.VMEM)
    hbm = pl.BlockSpec(memory_space=pl.ANY)
    rows = S * cap
    return pl.pallas_call(
        functools.partial(expert_kernel, S, T),
        name="expert_exchange",
        out_shape=(
            jax.ShapeDtypeStruct((S, cap, Q), bf),
            jax.ShapeDtypeStruct((S,) + out_gate.shape, bf),
            jax.ShapeDtypeStruct((D, H), bf),
            jax.ShapeDtypeStruct((D, H), bf),
            jax.ShapeDtypeStruct((H, D), bf),
        ),
        in_specs=[vmem] * 6 + [hbm] * 3,
        out_specs=(hbm,) * 5,
        scratch_shapes=[
            pltpu.VMEM(out_gate.shape, bf),
            pltpu.VMEM((2, S, T, cap, Q), bf),
            pltpu.VMEM((2, S, cap, Q), bf),
            pltpu.VMEM((D, 2 * H), bf),
            pltpu.VMEM((H, D), bf),
            pltpu.VMEM((S, cap, 2 * H), f32),
            pltpu.VMEM((S, cap, H), bf),
            pltpu.VMEM((S, cap, 2 * H), bf),
            pltpu.VMEM((2, 2, TH, cap, Q), f32),
            pltpu.VMEM((S, TH, cap, Q), f32),
            pltpu.VMEM((2, cap, Q), f32),
            pltpu.VMEM((2, TH, NEAR, cap, Q), bf),
            pltpu.VMEM((TH, S, cap, Q), bf),
            pltpu.VMEM((TH, S, cap, Q), bf),
            pltpu.VMEM((S, cap, Q), bf),
            pltpu.VMEM((D, 2 * H), bf),
            pltpu.VMEM((H, D), bf),
            dma((3,)), dma((4,)),
            dma((2, S)), dma((2, S)),
            dma((2, S)), dma((2, S)),
            dma((2, TH, S)), dma((2, TH, S)),
            dma((2, TH, S)), dma((2, TH, S)),
            dma((S,)), dma((S,)),
            dma((TH, S)), dma((TH, S)),
            dma((S,)), dma((S,)),
            dma((SH,)), dma((SH + 1,)),
            dma((SH,)), dma((SH + 1,)),
            dma((SH,)), dma((SH,)),
        ],
        cost_estimate=pl.CostEstimate(
            flops=16 * rows * D * H, bytes_accessed=8 * rows * D + 24 * D * H, transcendentals=rows * H
        ),
        compiler_params=pltpu.CompilerParams(
            collective_id=0, has_side_effects=True, vmem_limit_bytes=67_043_328
        ),
    )(inp, cot, placed, slot_w, out_gate, conv_out, w_gate, w_up, w_down)


def mixer(S, T, placed, cot, out_gate, conv_out, in_gate, conv_in, taps, back, mix_all, w_out):
    tok, D = cot.shape
    B = w_out.shape[1]
    cap = placed.shape[1]
    TH, Q = T // 2, D // T
    bf, f32 = jnp.bfloat16, jnp.float32
    dma = pltpu.SemaphoreType.DMA
    vmem = pl.BlockSpec(memory_space=pltpu.VMEM)
    hbm = pl.BlockSpec(memory_space=pl.ANY)
    small = jax.ShapeDtypeStruct((tok, B), bf)
    return pl.pallas_call(
        functools.partial(mixer_kernel, S, T),
        name="mixer",
        out_shape=(jax.ShapeDtypeStruct((D // S, B), f32), small, small, small),
        in_specs=[vmem] * 7 + [hbm] * 3,
        out_specs=(vmem,) * 4,
        scratch_shapes=[
            pltpu.VMEM((S, cap, Q), bf),
            pltpu.VMEM((S, tok, B), bf),
            pltpu.VMEM((D, B), bf),
            pltpu.VMEM((tok, Q), f32),
            pltpu.VMEM((T, tok, Q), bf),
            pltpu.VMEM((S, tok, Q // S), bf),
            pltpu.VMEM((S, T, tok, Q // S), bf),
            pltpu.VMEM((tok + 8, B), f32),
            pltpu.VMEM((8, B), f32),
            dma((3,)),
            dma((S,)), dma((S,)),
            dma((S + 1,)), dma((S + 1,)),
            dma((TH, S + 1)), dma((TH, S + 1)),
            dma((TH, S + 1)), dma((TH, S + 1)),
            dma((1,)), dma((1,)),
        ],
        cost_estimate=pl.CostEstimate(
            flops=2 * tok * D * B * 2 + 2 * S * cap * tok * Q, bytes_accessed=4 * D * B, transcendentals=0
        ),
        compiler_params=pltpu.CompilerParams(
            collective_id=1, has_side_effects=True, vmem_limit_bytes=67_043_328
        ),
    )(placed, cot, out_gate, conv_out, in_gate, conv_in, taps, back, mix_all, w_out)


def slot_masks(routes, route_weight, experts, capacity):
    tok_rows = routes.shape[0]
    names = jnp.arange(experts, dtype=jnp.int32)
    hits = routes[None, :, :] == names[:, None, None]
    chosen = jnp.any(hits, axis=2)
    weight = jnp.sum(jnp.where(hits, route_weight[None], 0.0), axis=2)
    order = jnp.arange(tok_rows, dtype=jnp.int32)
    before = (order[:, None] < order[None, :]).astype(jnp.bfloat16)
    rank = jnp.dot(chosen.astype(jnp.bfloat16), before, preferred_element_type=jnp.float32)
    rank = jnp.where(chosen, rank.astype(jnp.int32), -1)
    slots = jnp.arange(capacity, dtype=jnp.int32)
    placed = rank[:, None, :] == slots[None, :, None]
    slot_weight = jnp.sum(jnp.where(placed, weight[:, None, :], 0.0), axis=2, keepdims=True)
    return placed.astype(jnp.bfloat16), slot_weight


def per_device(
    cotangent, moe_input, routes, route_weight, conv_input, input_gate, output_gate, conv_output,
    taps, w_out, w_gate, w_up, w_down,
):
    experts = lax.axis_size("sp")
    tp_size = lax.axis_size("tp")
    tok_rows, top_k = routes.shape
    capacity = -(-max(2, 2 * tok_rows * top_k // experts) // 16) * 16
    placed, slot_weight = slot_masks(routes, route_weight, experts, capacity)
    returned, mixed_all, gate_wgrad, up_wgrad, grad_down = expert_exchange(
        experts, tp_size, capacity, moe_input, cotangent, placed, slot_weight, output_gate, conv_output,
        w_gate[0], w_up[0], w_down[0],
    )
    grad_w_out, grad_conv_input, grad_input_gate, grad_output_gate = mixer(
        experts, tp_size, placed, cotangent, output_gate, conv_output, input_gate, conv_input, taps,
        returned, mixed_all, w_out,
    )
    return (
        gate_wgrad[None], up_wgrad[None], grad_down[None], grad_w_out,
        grad_conv_input, grad_input_gate, grad_output_gate,
    )


def solution(mesh):
    return jax.shard_map(
        per_device,
        mesh=mesh,
        in_specs=(
            P("sp", None), P("sp", None), P("sp", None), P("sp", None),
            P("sp", "tp"), P("sp", "tp"), P("sp", "tp"), P("sp", "tp"),
            P(None, "tp"), P(None, "tp"),
            P("sp", None, "tp"), P("sp", None, "tp"), P("sp", "tp", None),
        ),
        out_specs=(
            P("sp", None, "tp"), P("sp", None, "tp"), P("sp", "tp", None),
            P("sp", "tp"), P("sp", "tp"), P("sp", "tp"), P("sp", "tp"),
        ),
        check_vma=False,
    )
```

```python
import functools

import jax
import jax.numpy as jnp
from jax import lax
from jax.experimental import pallas as pl
from jax.experimental.pallas import tpu as pltpu
from jax.sharding import PartitionSpec as P

NEAR = 4
LAG = 1
MESH = pl.DeviceIdType.MESH
NN = (((1,), (0,)), ((), ()))
NT = (((1,), (1,)), ((), ()))
TN = (((0,), (0,)), ((), ()))


def dot(a, b, dims=NN):
    return lax.dot_general(a, b, dims, preferred_element_type=jnp.float32)


def each(low, high, step):
    def body(i, carry):
        step(i)
        return carry

    lax.fori_loop(low, high, body, 0)


def spot():
    s, t = lax.axis_index("sp"), lax.axis_index("tp")
    return s, t, lax.div(t, 2), lax.rem(t, 2)


def flip(S, a, b):
    total, weight = 0, 1
    while weight < S:
        p, q = lax.rem(lax.div(a, weight), 2), lax.rem(lax.div(b, weight), 2)
        total, weight = total + (p + q - 2 * p * q) * weight, 2 * weight
    return total


def partner(S, s, i):
    if S < 4:
        return i
    high, low = lax.div(s, S // 2), lax.rem(lax.div(s, S // 4), 2)
    inner = high + low - 2 * high * low
    turned = S // 2 + lax.rem(i - S // 2 + inner * (S // 4) + S, S // 2)
    return jnp.where(i >= S // 2, turned, i)


def remote(src, dst, send, recv, device):
    return pltpu.make_async_remote_copy(
        src_ref=src, dst_ref=dst, send_sem=send, recv_sem=recv, device_id=device, device_id_type=MESH
    )


def greet(S, TH):
    s, t, th, tl = spot()
    barrier = pltpu.get_barrier_semaphore()

    def hello(device):
        pl.semaphore_signal(barrier, inc=1, device_id=device, device_id_type=MESH)

    each(1, S, lambda k: hello((lax.rem(s + k, S), t)))
    hello((s, 2 * th + 1 - tl))
    for j in range(1, TH):
        hello((s, 2 * lax.rem(th + j, TH) + tl))
    pl.semaphore_wait(barrier, S - 1 + TH)


def expert_kernel(
    S, T, inp, cot, placed, slot_w, out_gate, conv_out, wg_h, wu_h, wd_h,
    back, mix_all, gwg_h, gwu_h, gwd_h,
    mix, rows, stage, wgu, wd, proj, hid, ggu, part, matebuf, total_part, near, xsend, xrecv, rstage, gout, gdown,
    wsem, gsem, ds, dr, m1s, m1r, xs, xr, m2s, m2r, r1s, r1r, r2s, r2r, rts, rtr, us, ur, vs, vr, ys, yr,
):
    TH = T // 2
    cap, Q = rows.shape[3], rows.shape[4]
    D = T * Q
    H = wd.shape[0]
    piece = Q // S
    group = D // S
    s, t, th, tl = spot()
    mate = 2 * th + 1 - tl
    source = (inp, cot)

    def other(j):
        return lax.rem(th + j, TH)

    def behind(j):
        return lax.rem(th - j + TH, TH)

    def src_of(k):
        return flip(S, s, k)

    def at(i):
        return partner(S, s, i)

    def then(i):
        far = S - S // 2
        return jnp.where(i <= far, at(i + S // 2 - 1), at(i - far))

    weights = [
        pltpu.make_async_copy(wg_h, wgu.at[:, pl.ds(0, H)], wsem.at[0]),
        pltpu.make_async_copy(wu_h, wgu.at[:, pl.ds(H, H)], wsem.at[1]),
        pltpu.make_async_copy(wd_h, wd, wsem.at[2]),
    ]
    for copy in weights:
        copy.start()
    greet(S, TH)

    def direct(a, k):
        return remote(stage.at[a, k], rows.at[a, s, t], ds.at[a, k], dr.at[a, k], (src_of(k), t))

    def direct_too(a, j, k):
        q = 2 * other(j) + tl
        return remote(near.at[a, j, k], rows.at[a, s, q], xs.at[a, j, k], xr.at[a, TH - j, k], (src_of(k), t))

    def to_mate(a, k):
        block = rows.at[a, src_of(k), t]
        return remote(block, block, m1s.at[a, k], m1r.at[a, k], (s, mate))

    def across(a, j, k):
        block = rows.at[a, src_of(k), t]
        return remote(block, block, xs.at[a, j, k], xr.at[a, j, k], (s, 2 * other(j) + tl))

    def on_to_mate(a, j, k):
        block = rows.at[a, src_of(k), 2 * behind(j) + tl]
        return remote(block, block, m2s.at[a, j, k], m2r.at[a, j, k], (s, mate))

    def pick(a, e, columns):
        picked = dot(placed[e], source[a][:, columns])
        if a == 1:
            picked = picked * slot_w[e]
        return picked.astype(jnp.bfloat16)

    def send(a, k):
        stage[a, k] = pick(a, src_of(k), pl.ds(pl.multiple_of(t * Q, Q), Q))
        direct(a, k).start()

        @pl.when(k < NEAR)
        def _():
            for j in range(1, TH):
                near[a, j, k] = pick(a, src_of(k), pl.ds(pl.multiple_of((2 * other(j) + tl) * Q, Q), Q))
                direct_too(a, j, k).start()

    def own(a):
        for q in range(T):
            rows[a, s, q] = pick(a, s, pl.ds(q * Q, Q))

    def forward(a, k):
        direct(a, k).wait_recv()

        @pl.when(k >= NEAR)
        def _():
            for j in range(1, TH):
                across(a, j, k).start()

        to_mate(a, k).start()

    def forward_on(a, k):
        for j in range(1, TH):
            across(a, j, k).wait_recv()
            on_to_mate(a, j, k).start()

    def complete(a, k):
        to_mate(a, k).wait_recv()
        for j in range(1, TH):
            on_to_mate(a, j, k).wait_recv()

    def project(k):
        b = src_of(k)
        total = dot(rows[0, b, 0], wgu[pl.ds(0, Q), :])
        for q in range(1, T):
            total = total + dot(rows[0, b, q], wgu[pl.ds(q * Q, Q), :])
        proj[b] = total

    def half(n):
        return remote(part.at[lax.rem(n, 2), 1 - tl], matebuf.at[n], r1s.at[n], r1r.at[n], (s, mate))

    def chip_sum(j, k):
        return remote(xsend.at[j, k], xrecv.at[j, k], r2s.at[j, k], r2r.at[j, k], (s, 2 * other(j) + tl))

    def give_back(k):
        return remote(rstage.at[k], back.at[s], rts.at[k], rtr.at[k], (src_of(k), t))

    def gradients(n, k):
        b = src_of(k)
        grad_hidden = dot(rows[1, b, 0], wd[:, pl.ds(0, Q)], NT)
        for q in range(1, T):
            grad_hidden = grad_hidden + dot(rows[1, b, q], wd[:, pl.ds(q * Q, Q)], NT)
        gate, up = proj[b][:, :H], proj[b][:, H:]
        sig = jax.nn.sigmoid(gate)
        act = gate * sig
        slope = sig * (1.0 + gate * (1.0 - sig))
        hid[b] = (act * up).astype(jnp.bfloat16)
        ggu[b, :, pl.ds(0, H)] = (grad_hidden * up * slope).astype(jnp.bfloat16)
        ggu[b, :, pl.ds(H, H)] = (grad_hidden * act).astype(jnp.bfloat16)

        @pl.when(n >= 2)
        def _():
            half(n - 2).wait_send()

        slot = lax.rem(n, 2)
        grads = ggu[b]
        for g in range(S):
            some = dot(grads, wgu[pl.ds(g * group, group), :], NT)
            for q in range(T):
                part[slot, q % 2, q // 2, :, pl.ds(g * piece, piece)] = some[:, q * piece : (q + 1) * piece]
        half(n).start()

    def reduce_chip(n, k):
        half(n).wait_recv()
        slot = lax.rem(n, 2)
        for j in range(1, TH):
            o = other(j)
            xsend[j, k] = (part[slot, tl, o] + matebuf[n, o]).astype(jnp.bfloat16)
            chip_sum(j, k).start()
        total_part[lax.rem(n, 3)] = part[slot, tl, th] + matebuf[n, th]

    def reduce_all(n, k):
        total = total_part[lax.rem(n, 3)]
        for j in range(1, TH):
            chip_sum(j, k).wait_recv()
            total = total + xrecv[j, k].astype(jnp.float32)
        rstage[k] = total.astype(jnp.bfloat16)

        @pl.when(k >= 1)
        def _():
            give_back(k).start()

    SH = S // 2
    sh, sl = lax.div(s, 2), lax.rem(s, 2)

    def block(h):
        return mix_all.at[2 * h + sl]

    def rise(j):
        return remote(mix if j == 0 else block(sh - j), block(sh - j), us.at[j], ur.at[j + 1], (s + 2, t))

    def sink(j):
        return remote(mix if j == 0 else block(sh + j), block(sh + j), vs.at[j], vr.at[j + 1], (s - 2, t))

    def side(h, value=None):
        return remote(block(h) if value is None else value, block(h), ys.at[h], yr.at[h], (2 * sh + 1 - sl, t))

    def mix_step(j):
        if j == 0:
            side(sh, mix).start()

            @pl.when(sh < SH - 1)
            def _():
                rise(0).start()

            @pl.when(sh > 0)
            def _():
                sink(0).start()

            return

        @pl.when(sh >= j)
        def _():
            remote(block(sh - j), block(sh - j), us.at[j], ur.at[j], (s, mate)).wait_recv()

            @pl.when(sh < SH - 1)
            def _():
                rise(j).start()

            side(sh - j).start()

        @pl.when(sh + j < SH)
        def _():
            remote(block(sh + j), block(sh + j), vs.at[j], vr.at[j], (s, mate)).wait_recv()

            @pl.when(sh > 0)
            def _():
                sink(j).start()

            side(sh + j).start()

    def mix_finish():
        keep_mix.wait()
        for j in range(SH - 1):

            @pl.when((sh >= j) & (sh < SH - 1))
            def _():
                rise(j).wait_send()

            @pl.when((sh + j < SH) & (sh > 0))
            def _():
                sink(j).wait_send()

        def one(h):
            side(h).wait_send()
            side(h).wait_recv()

        each(0, SH, one)

    keep_mix = pltpu.make_async_copy(mix, mix_all.at[s], gsem.at[3])
    keep = pltpu.make_async_copy(rstage.at[0], back.at[s], rts.at[0])

    each(1, S, lambda i: send(0, at(i)))
    own(0)
    mix[...] = (out_gate[...].astype(jnp.float32) * conv_out[...].astype(jnp.float32)).astype(jnp.bfloat16)
    own(1)
    for copy in weights:
        copy.wait()
    project(0)
    gradients(0, 0)

    def first(i):
        @pl.when(i == 3)
        def _():
            reduce_chip(0, 0)

        @pl.when(i == 4)
        def _():
            reduce_all(0, 0)

        @pl.when(i < S)
        def _():
            forward(0, at(i))

        @pl.when((i >= LAG) & (i < S))
        def _():
            send(1, then(i - LAG + 1))

        @pl.when((i >= 2) & (i < S + 1))
        def _():
            forward_on(0, at(i - 1))

        @pl.when(i >= 3)
        def _():
            complete(0, at(i - 2))
            project(at(i - 2))

    each(1, S + 2, first)
    each(max(1, S - LAG + 1), S, lambda i: send(1, then(i)))
    mix_step(0)

    def second(i):
        @pl.when(i < S)
        def _():
            forward(1, then(i))

        @pl.when((i >= 2) & (i < S + 1))
        def _():
            forward_on(1, then(i - 1))

        @pl.when((i >= 3) & (i < S + 2))
        def _():
            complete(1, then(i - 2))
            gradients(i - 2, then(i - 2))

        @pl.when((i >= 4) & (i < S + 3))
        def _():
            reduce_chip(i - 3, then(i - 3))

        @pl.when(i >= 6)
        def _():
            reduce_all(i - 5, then(i - 5))

        for j in range(1, SH):

            @pl.when(i == 2 * j)
            def _():
                mix_step(j)

    each(1, S + 5, second)
    keep.start()
    keep_mix.start()

    tile = min(512, Q)
    per = Q // tile

    def weight_grads(i):
        q, c = lax.div(i, per), pl.multiple_of(lax.rem(i, per) * tile, tile)
        x = rows[0, :, q, :, pl.ds(c, tile)].reshape(S * cap, tile)
        start = pl.multiple_of(q * Q + c, tile)
        gout[pl.ds(start, tile), :] = dot(x, ggu[...].reshape(S * cap, 2 * H), TN).astype(jnp.bfloat16)
        d = rows[1, :, q, :, pl.ds(c, tile)].reshape(S * cap, tile)
        gdown[:, pl.ds(start, tile)] = dot(hid[...].reshape(S * cap, H), d, TN).astype(jnp.bfloat16)

    each(0, T * per, weight_grads)
    results = [
        pltpu.make_async_copy(gout.at[:, pl.ds(0, H)], gwg_h, gsem.at[0]),
        pltpu.make_async_copy(gout.at[:, pl.ds(H, H)], gwu_h, gsem.at[1]),
        pltpu.make_async_copy(gdown, gwd_h, gsem.at[2]),
    ]
    for copy in results:
        copy.start()

    half(S - 2).wait_send()
    half(S - 1).wait_send()

    def finish(k):
        for a in range(2):
            direct(a, k).wait_send()
            to_mate(a, k).wait_send()
            for j in range(1, TH):
                across(a, j, k).wait_send()
                on_to_mate(a, j, k).wait_send()
        give_back(k).wait_send()
        give_back(k).wait_recv()

    each(1, S, finish)

    def finish_sums(k):
        for j in range(1, TH):
            chip_sum(j, k).wait_send()

    each(0, S, finish_sums)
    keep.wait()
    mix_finish()
    for copy in results:
        copy.wait()


def mixer_kernel(
    S, T, placed, cot, out_gate, conv_out, in_gate, conv_in, taps, back_h, mix_h, w_out_h,
    gwo, gci, gig, gog,
    back, mix, w_out, total, res, colst, cols, conv, after,
    lsem, ds, dr, m1s, m1r, xs, xr, m2s, m2r, bs, br,
):
    TH = T // 2
    cap, Q = back.shape[1], back.shape[2]
    tok = cot.shape[0]
    piece, group = Q // S, T * Q // S
    s, t, th, tl = spot()
    mate = 2 * th + 1 - tl
    local = [
        pltpu.make_async_copy(src, dst, lsem.at[n])
        for n, (src, dst) in enumerate(((back_h, back), (mix_h, mix), (w_out_h, w_out)))
    ]
    for copy in local:
        copy.start()
    greet(S, TH)

    def other(j):
        return lax.rem(th + j, TH)

    def behind(j):
        return lax.rem(th - j + TH, TH)

    def at(i):
        return partner(S, s, i)

    def direct(k):
        peer = flip(S, s, k)
        return remote(colst.at[peer], cols.at[s, t], ds.at[k], dr.at[k], (peer, t))

    def block(k, q):
        return cols.at[flip(S, s, k), q] if k is not None else res.at[q]

    def to_mate(k):
        n = S if k is None else k
        return remote(block(k, t), block(k, t), m1s.at[n], m1r.at[n], (s, mate))

    def across(j, k):
        n = S if k is None else k
        return remote(block(k, t), block(k, t), xs.at[j, n], xr.at[j, n], (s, 2 * other(j) + tl))

    def on_to_mate(j, k):
        n = S if k is None else k
        q = 2 * behind(j) + tl
        return remote(block(k, q), block(k, q), m2s.at[j, n], m2r.at[j, n], (s, mate))

    def forward(k):
        for j in range(1, TH):
            across(j, k).start()
        to_mate(k).start()

    def forward_on(k):
        for j in range(1, TH):
            across(j, k).wait_recv()
            on_to_mate(j, k).start()

    def complete(k):
        to_mate(k).wait_recv()
        for j in range(1, TH):
            on_to_mate(j, k).wait_recv()

    def sent(k):
        to_mate(k).wait_send()
        for j in range(1, TH):
            across(j, k).wait_send()
            on_to_mate(j, k).wait_send()

    local[0].wait()
    total[...] = dot(placed[...].reshape(S * cap, tok), back[...].reshape(S * cap, Q), TN)
    for q in range(T):

        @pl.when(t == q)
        def _():
            for g in range(S):
                columns = pl.ds(g * piece, piece)
                mine = cot[:, pl.ds(g * group + q * piece, piece)].astype(jnp.float32)
                value = (mine + total[:, columns]).astype(jnp.bfloat16)
                res[q, :, columns] = value
                colst[g] = value

    forward(None)
    each(1, S, lambda i: direct(at(i)).start())
    cols[s, t] = colst[s]
    forward(0)

    def arrive(i):
        direct(at(i)).wait_recv()
        forward(at(i))

    local[2].wait()
    forward_on(None)
    each(1, S, arrive)
    complete(None)
    grad_mixed = jnp.zeros((tok, w_out.shape[1]), jnp.float32)
    for g in range(S):
        some = jnp.concatenate([res[q, :, pl.ds(g * piece, piece)] for q in range(T)], axis=1)
        grad_mixed = grad_mixed + dot(some, w_out[pl.ds(g * group, group), :])
    gog[...] = (grad_mixed * conv_out[...].astype(jnp.float32)).astype(jnp.bfloat16)
    conv[pl.ds(0, tok), :] = grad_mixed * out_gate[...].astype(jnp.float32)

    def edge(target):
        return remote(conv.at[pl.ds(0, 8), :], after, bs.at[0], br.at[0], (target, t))

    @pl.when(s > 0)
    def _():
        edge(s - 1).start()

    local[1].wait()

    def take(k):
        complete(k)
        b = flip(S, s, k)
        columns = jnp.concatenate([cols[b, q] for q in range(T)], axis=1)
        gwo[...] += dot(columns, mix[b], TN)

    gwo[...] = jnp.zeros_like(gwo)
    forward_on(0)

    def step(i):
        @pl.when(i < S)
        def _():
            forward_on(at(i))

        take(at(i - 1))

    each(1, S + 1, step)

    @pl.when(s < S - 1)
    def _():
        edge(0).wait_recv()
        conv[pl.ds(tok, 8), :] = after[...]

    @pl.when(s == S - 1)
    def _():
        conv[pl.ds(tok, 8), :] = jnp.zeros_like(after)

    grad_g = (
        taps[2:3, :] * conv[pl.ds(0, tok), :]
        + taps[1:2, :] * conv[pl.ds(1, tok), :]
        + taps[0:1, :] * conv[pl.ds(2, tok), :]
    )
    gci[...] = (grad_g * in_gate[...].astype(jnp.float32)).astype(jnp.bfloat16)
    gig[...] = (grad_g * conv_in[...].astype(jnp.float32)).astype(jnp.bfloat16)

    @pl.when(s > 0)
    def _():
        edge(s - 1).wait_send()

    sent(None)
    each(0, S, sent)
    each(1, S, lambda k: direct(k).wait_send())


def expert_exchange(S, T, cap, inp, cot, placed, slot_w, out_gate, conv_out, w_gate, w_up, w_down):
    tok, D = inp.shape
    H = w_down.shape[0]
    TH, Q, SH = T // 2, D // T, S // 2
    bf, f32 = jnp.bfloat16, jnp.float32
    dma = pltpu.SemaphoreType.DMA
    vmem = pl.BlockSpec(memory_space=pltpu.VMEM)
    hbm = pl.BlockSpec(memory_space=pl.ANY)
    rows = S * cap
    return pl.pallas_call(
        functools.partial(expert_kernel, S, T),
        name="expert_exchange",
        out_shape=(
            jax.ShapeDtypeStruct((S, cap, Q), bf),
            jax.ShapeDtypeStruct((S,) + out_gate.shape, bf),
            jax.ShapeDtypeStruct((D, H), bf),
            jax.ShapeDtypeStruct((D, H), bf),
            jax.ShapeDtypeStruct((H, D), bf),
        ),
        in_specs=[vmem] * 6 + [hbm] * 3,
        out_specs=(hbm,) * 5,
        scratch_shapes=[
            pltpu.VMEM(out_gate.shape, bf),
            pltpu.VMEM((2, S, T, cap, Q), bf),
            pltpu.VMEM((2, S, cap, Q), bf),
            pltpu.VMEM((D, 2 * H), bf),
            pltpu.VMEM((H, D), bf),
            pltpu.VMEM((S, cap, 2 * H), f32),
            pltpu.VMEM((S, cap, H), bf),
            pltpu.VMEM((S, cap, 2 * H), bf),
            pltpu.VMEM((2, 2, TH, cap, Q), f32),
            pltpu.VMEM((S, TH, cap, Q), f32),
            pltpu.VMEM((3, cap, Q), f32),
            pltpu.VMEM((2, TH, NEAR, cap, Q), bf),
            pltpu.VMEM((TH, S, cap, Q), bf),
            pltpu.VMEM((TH, S, cap, Q), bf),
            pltpu.VMEM((S, cap, Q), bf),
            pltpu.VMEM((D, 2 * H), bf),
            pltpu.VMEM((H, D), bf),
            dma((3,)), dma((4,)),
            dma((2, S)), dma((2, S)),
            dma((2, S)), dma((2, S)),
            dma((2, TH, S)), dma((2, TH, S)),
            dma((2, TH, S)), dma((2, TH, S)),
            dma((S,)), dma((S,)),
            dma((TH, S)), dma((TH, S)),
            dma((S,)), dma((S,)),
            dma((SH,)), dma((SH + 1,)),
            dma((SH,)), dma((SH + 1,)),
            dma((SH,)), dma((SH,)),
        ],
        cost_estimate=pl.CostEstimate(
            flops=16 * rows * D * H, bytes_accessed=8 * rows * D + 24 * D * H, transcendentals=rows * H
        ),
        compiler_params=pltpu.CompilerParams(
            collective_id=0, has_side_effects=True, vmem_limit_bytes=67_043_328
        ),
    )(inp, cot, placed, slot_w, out_gate, conv_out, w_gate, w_up, w_down)


def mixer(S, T, placed, cot, out_gate, conv_out, in_gate, conv_in, taps, back, mix_all, w_out):
    tok, D = cot.shape
    B = w_out.shape[1]
    cap = placed.shape[1]
    TH, Q = T // 2, D // T
    bf, f32 = jnp.bfloat16, jnp.float32
    dma = pltpu.SemaphoreType.DMA
    vmem = pl.BlockSpec(memory_space=pltpu.VMEM)
    hbm = pl.BlockSpec(memory_space=pl.ANY)
    small = jax.ShapeDtypeStruct((tok, B), bf)
    return pl.pallas_call(
        functools.partial(mixer_kernel, S, T),
        name="mixer",
        out_shape=(jax.ShapeDtypeStruct((D // S, B), f32), small, small, small),
        in_specs=[vmem] * 7 + [hbm] * 3,
        out_specs=(vmem,) * 4,
        scratch_shapes=[
            pltpu.VMEM((S, cap, Q), bf),
            pltpu.VMEM((S, tok, B), bf),
            pltpu.VMEM((D, B), bf),
            pltpu.VMEM((tok, Q), f32),
            pltpu.VMEM((T, tok, Q), bf),
            pltpu.VMEM((S, tok, Q // S), bf),
            pltpu.VMEM((S, T, tok, Q // S), bf),
            pltpu.VMEM((tok + 8, B), f32),
            pltpu.VMEM((8, B), f32),
            dma((3,)),
            dma((S,)), dma((S,)),
            dma((S + 1,)), dma((S + 1,)),
            dma((TH, S + 1)), dma((TH, S + 1)),
            dma((TH, S + 1)), dma((TH, S + 1)),
            dma((1,)), dma((1,)),
        ],
        cost_estimate=pl.CostEstimate(
            flops=2 * tok * D * B * 2 + 2 * S * cap * tok * Q, bytes_accessed=4 * D * B, transcendentals=0
        ),
        compiler_params=pltpu.CompilerParams(
            collective_id=1, has_side_effects=True, vmem_limit_bytes=67_043_328
        ),
    )(placed, cot, out_gate, conv_out, in_gate, conv_in, taps, back, mix_all, w_out)


def slot_masks(routes, route_weight, experts, capacity):
    tok_rows = routes.shape[0]
    names = jnp.arange(experts, dtype=jnp.int32)
    hits = routes[None, :, :] == names[:, None, None]
    chosen = jnp.any(hits, axis=2)
    weight = jnp.sum(jnp.where(hits, route_weight[None], 0.0), axis=2)
    order = jnp.arange(tok_rows, dtype=jnp.int32)
    before = (order[:, None] < order[None, :]).astype(jnp.bfloat16)
    rank = jnp.dot(chosen.astype(jnp.bfloat16), before, preferred_element_type=jnp.float32)
    rank = jnp.where(chosen, rank.astype(jnp.int32), -1)
    slots = jnp.arange(capacity, dtype=jnp.int32)
    placed = rank[:, None, :] == slots[None, :, None]
    slot_weight = jnp.sum(jnp.where(placed, weight[:, None, :], 0.0), axis=2, keepdims=True)
    return placed.astype(jnp.bfloat16), slot_weight


def per_device(
    cotangent, moe_input, routes, route_weight, conv_input, input_gate, output_gate, conv_output,
    taps, w_out, w_gate, w_up, w_down,
):
    experts = lax.axis_size("sp")
    tp_size = lax.axis_size("tp")
    tok_rows, top_k = routes.shape
    capacity = -(-max(2, 2 * tok_rows * top_k // experts) // 16) * 16
    placed, slot_weight = slot_masks(routes, route_weight, experts, capacity)
    returned, mixed_all, gate_wgrad, up_wgrad, grad_down = expert_exchange(
        experts, tp_size, capacity, moe_input, cotangent, placed, slot_weight, output_gate, conv_output,
        w_gate[0], w_up[0], w_down[0],
    )
    grad_w_out, grad_conv_input, grad_input_gate, grad_output_gate = mixer(
        experts, tp_size, placed, cotangent, output_gate, conv_output, input_gate, conv_input, taps,
        returned, mixed_all, w_out,
    )
    return (
        gate_wgrad[None], up_wgrad[None], grad_down[None], grad_w_out,
        grad_conv_input, grad_input_gate, grad_output_gate,
    )


def solution(mesh):
    return jax.shard_map(
        per_device,
        mesh=mesh,
        in_specs=(
            P("sp", None), P("sp", None), P("sp", None), P("sp", None),
            P("sp", "tp"), P("sp", "tp"), P("sp", "tp"), P("sp", "tp"),
            P(None, "tp"), P(None, "tp"),
            P("sp", None, "tp"), P("sp", None, "tp"), P("sp", "tp", None),
        ),
        out_specs=(
            P("sp", None, "tp"), P("sp", None, "tp"), P("sp", "tp", None),
            P("sp", "tp"), P("sp", "tp"), P("sp", "tp"), P("sp", "tp"),
        ),
        check_vma=False,
    )
```

```python
import functools

import jax
import jax.numpy as jnp
from jax import lax
from jax.experimental import pallas as pl
from jax.experimental.pallas import tpu as pltpu
from jax.sharding import PartitionSpec as P

NEAR = 4
MESH = pl.DeviceIdType.MESH
NN = (((1,), (0,)), ((), ()))
NT = (((1,), (1,)), ((), ()))
TN = (((0,), (0,)), ((), ()))


def dot(a, b, dims=NN):
    return lax.dot_general(a, b, dims, preferred_element_type=jnp.float32)


def each(low, high, step):
    def body(i, carry):
        step(i)
        return carry

    lax.fori_loop(low, high, body, 0)


def spot():
    s, t = lax.axis_index("sp"), lax.axis_index("tp")
    return s, t, lax.div(t, 2), lax.rem(t, 2)


def flip(S, a, b):
    total, weight = 0, 1
    while weight < S:
        p, q = lax.rem(lax.div(a, weight), 2), lax.rem(lax.div(b, weight), 2)
        total, weight = total + (p + q - 2 * p * q) * weight, 2 * weight
    return total


def partner(S, s, i):
    if S < 4:
        return i
    high, low = lax.div(s, S // 2), lax.rem(lax.div(s, S // 4), 2)
    inner = high + low - 2 * high * low
    turned = S // 2 + lax.rem(i - S // 2 + inner * (S // 4) + S, S // 2)
    return jnp.where(i >= S // 2, turned, i)


def remote(src, dst, send, recv, device):
    return pltpu.make_async_remote_copy(
        src_ref=src, dst_ref=dst, send_sem=send, recv_sem=recv, device_id=device, device_id_type=MESH
    )


def greet(S, TH):
    s, t, th, tl = spot()
    barrier = pltpu.get_barrier_semaphore()

    def hello(device):
        pl.semaphore_signal(barrier, inc=1, device_id=device, device_id_type=MESH)

    each(1, S, lambda k: hello((lax.rem(s + k, S), t)))
    hello((s, 2 * th + 1 - tl))
    for j in range(1, TH):
        hello((s, 2 * lax.rem(th + j, TH) + tl))
    pl.semaphore_wait(barrier, S - 1 + TH)


def expert_kernel(
    S, T, inp, cot, placed, slot_w, out_gate, conv_out, wg_h, wu_h, wd_h,
    back, mix_all, gwg_h, gwu_h, gwd_h,
    mix, rows, stage, wgu, wd, proj, hid, ggu, part, matebuf, total_part, near, xsend, xrecv, rstage, gout, gdown,
    wsem, gsem, ds, dr, m1s, m1r, xs, xr, m2s, m2r, r1s, r1r, r2s, r2r, rts, rtr, us, ur, vs, vr, ys, yr,
):
    TH = T // 2
    cap, Q = rows.shape[3], rows.shape[4]
    D = T * Q
    H = wd.shape[0]
    piece = Q // S
    group = D // S
    s, t, th, tl = spot()
    mate = 2 * th + 1 - tl
    source = (inp, cot)

    def other(j):
        return lax.rem(th + j, TH)

    def behind(j):
        return lax.rem(th - j + TH, TH)

    def src_of(k):
        return flip(S, s, k)

    def at(i):
        return partner(S, s, i)

    weights = [
        pltpu.make_async_copy(wg_h, wgu.at[:, pl.ds(0, H)], wsem.at[0]),
        pltpu.make_async_copy(wu_h, wgu.at[:, pl.ds(H, H)], wsem.at[1]),
        pltpu.make_async_copy(wd_h, wd, wsem.at[2]),
    ]
    for copy in weights:
        copy.start()
    greet(S, TH)

    def direct(a, k):
        return remote(stage.at[a, k], rows.at[a, s, t], ds.at[a, k], dr.at[a, k], (src_of(k), t))

    def direct_too(a, j, k):
        q = 2 * other(j) + tl
        return remote(near.at[a, j, k], rows.at[a, s, q], xs.at[a, j, k], xr.at[a, TH - j, k], (src_of(k), t))

    def to_mate(a, k):
        block = rows.at[a, src_of(k), t]
        return remote(block, block, m1s.at[a, k], m1r.at[a, k], (s, mate))

    def across(a, j, k):
        block = rows.at[a, src_of(k), t]
        return remote(block, block, xs.at[a, j, k], xr.at[a, j, k], (s, 2 * other(j) + tl))

    def on_to_mate(a, j, k):
        block = rows.at[a, src_of(k), 2 * behind(j) + tl]
        return remote(block, block, m2s.at[a, j, k], m2r.at[a, j, k], (s, mate))

    def pick(a, e, columns):
        picked = dot(placed[e], source[a][:, columns])
        if a == 1:
            picked = picked * slot_w[e]
        return picked.astype(jnp.bfloat16)

    def send(a, k):
        stage[a, k] = pick(a, src_of(k), pl.ds(pl.multiple_of(t * Q, Q), Q))
        direct(a, k).start()

        @pl.when(k < NEAR)
        def _():
            for j in range(1, TH):
                near[a, j, k] = pick(a, src_of(k), pl.ds(pl.multiple_of((2 * other(j) + tl) * Q, Q), Q))
                direct_too(a, j, k).start()

    def own(a):
        for q in range(T):
            rows[a, s, q] = pick(a, s, pl.ds(q * Q, Q))

    def forward(a, k):
        direct(a, k).wait_recv()

        @pl.when(k >= NEAR)
        def _():
            for j in range(1, TH):
                across(a, j, k).start()

        to_mate(a, k).start()

    def forward_on(a, k):
        for j in range(1, TH):
            across(a, j, k).wait_recv()
            on_to_mate(a, j, k).start()

    def complete(a, k):
        to_mate(a, k).wait_recv()
        for j in range(1, TH):
            on_to_mate(a, j, k).wait_recv()

    def project(k):
        b = src_of(k)
        total = dot(rows[0, b, 0], wgu[pl.ds(0, Q), :])
        for q in range(1, T):
            total = total + dot(rows[0, b, q], wgu[pl.ds(q * Q, Q), :])
        proj[b] = total

    def half(n):
        return remote(part.at[lax.rem(n, 2), 1 - tl], matebuf.at[n], r1s.at[n], r1r.at[n], (s, mate))

    def chip_sum(j, k):
        return remote(xsend.at[j, k], xrecv.at[j, k], r2s.at[j, k], r2r.at[j, k], (s, 2 * other(j) + tl))

    def give_back(k):
        return remote(rstage.at[k], back.at[s], rts.at[k], rtr.at[k], (src_of(k), t))

    def gradients(n, k):
        b = src_of(k)
        grad_hidden = dot(rows[1, b, 0], wd[:, pl.ds(0, Q)], NT)
        for q in range(1, T):
            grad_hidden = grad_hidden + dot(rows[1, b, q], wd[:, pl.ds(q * Q, Q)], NT)
        gate, up = proj[b][:, :H], proj[b][:, H:]
        sig = jax.nn.sigmoid(gate)
        act = gate * sig
        slope = sig * (1.0 + gate * (1.0 - sig))
        hid[b] = (act * up).astype(jnp.bfloat16)
        ggu[b, :, pl.ds(0, H)] = (grad_hidden * up * slope).astype(jnp.bfloat16)
        ggu[b, :, pl.ds(H, H)] = (grad_hidden * act).astype(jnp.bfloat16)

        @pl.when(n >= 2)
        def _():
            half(n - 2).wait_send()

        slot = lax.rem(n, 2)
        grads = ggu[b]
        for g in range(S):
            some = dot(grads, wgu[pl.ds(g * group, group), :], NT)
            for q in range(T):
                part[slot, q % 2, q // 2, :, pl.ds(g * piece, piece)] = some[:, q * piece : (q + 1) * piece]
        half(n).start()

    def reduce_chip(n, k):
        half(n).wait_recv()
        slot = lax.rem(n, 2)
        for j in range(1, TH):
            o = other(j)
            xsend[j, k] = (part[slot, tl, o] + matebuf[n, o]).astype(jnp.bfloat16)
            chip_sum(j, k).start()
        total_part[lax.rem(n, 3)] = part[slot, tl, th] + matebuf[n, th]

    def reduce_all(n, k):
        total = total_part[lax.rem(n, 3)]
        for j in range(1, TH):
            chip_sum(j, k).wait_recv()
            total = total + xrecv[j, k].astype(jnp.float32)
        rstage[k] = total.astype(jnp.bfloat16)

        @pl.when(k >= 1)
        def _():
            give_back(k).start()

    SH = S // 2
    sh, sl = lax.div(s, 2), lax.rem(s, 2)

    def block(h):
        return mix_all.at[2 * h + sl]

    def rise(j):
        return remote(mix if j == 0 else block(sh - j), block(sh - j), us.at[j], ur.at[j + 1], (s + 2, t))

    def sink(j):
        return remote(mix if j == 0 else block(sh + j), block(sh + j), vs.at[j], vr.at[j + 1], (s - 2, t))

    def side(h, value=None):
        return remote(block(h) if value is None else value, block(h), ys.at[h], yr.at[h], (2 * sh + 1 - sl, t))

    def mix_step(j):
        if j == 0:
            side(sh, mix).start()

            @pl.when(sh < SH - 1)
            def _():
                rise(0).start()

            @pl.when(sh > 0)
            def _():
                sink(0).start()

            return

        @pl.when(sh >= j)
        def _():
            remote(block(sh - j), block(sh - j), us.at[j], ur.at[j], (s, mate)).wait_recv()

            @pl.when(sh < SH - 1)
            def _():
                rise(j).start()

            side(sh - j).start()

        @pl.when(sh + j < SH)
        def _():
            remote(block(sh + j), block(sh + j), vs.at[j], vr.at[j], (s, mate)).wait_recv()

            @pl.when(sh > 0)
            def _():
                sink(j).start()

            side(sh + j).start()

    def mix_finish():
        keep_mix.wait()
        for j in range(SH - 1):

            @pl.when((sh >= j) & (sh < SH - 1))
            def _():
                rise(j).wait_send()

            @pl.when((sh + j < SH) & (sh > 0))
            def _():
                sink(j).wait_send()

        def one(h):
            side(h).wait_send()
            side(h).wait_recv()

        each(0, SH, one)

    keep_mix = pltpu.make_async_copy(mix, mix_all.at[s], gsem.at[3])
    keep = pltpu.make_async_copy(rstage.at[0], back.at[s], rts.at[0])

    mix[...] = (out_gate[...].astype(jnp.float32) * conv_out[...].astype(jnp.float32)).astype(jnp.bfloat16)
    middle = max(2, S // 2)
    each(middle, S, lambda i: send(0, at(i)))
    mix_step(0)
    each(1, middle, lambda i: send(0, at(i)))
    each(1, middle, lambda i: send(1, at(i)))
    own(0)
    own(1)
    for copy in weights:
        copy.wait()
    project(0)
    gradients(0, 0)

    def first(i):
        @pl.when(i < S)
        def _():
            forward(0, at(i))

        @pl.when(i == S - 1)
        def _():
            each(middle, S, lambda m: send(1, at(m)))

        @pl.when(i == middle + 1)
        def _():
            reduce_chip(0, 0)

        @pl.when(i == middle + 3)
        def _():
            reduce_all(0, 0)

        @pl.when((i >= middle + 1) & (i < S + 1))
        def _():
            forward_on(0, at(i - 1))

        @pl.when(i >= middle + 2)
        def _():
            complete(0, at(i - 2))
            project(at(i - 2))

    each(middle, S + 2, first)
    mix_step(1)

    lead = S // 4

    def near_at(i):
        return (i > lead) & (i < lead + middle)

    def then(i):
        return jnp.where(i <= lead, at(i + middle - 1), jnp.where(i < lead + middle, at(i - lead), at(i)))

    def second(i):
        @pl.when(near_at(i))
        def _():
            forward(0, then(i))

        @pl.when(i < S)
        def _():
            forward(1, then(i))

        @pl.when(near_at(i - 1))
        def _():
            forward_on(0, then(i - 1))

        @pl.when((i >= 2) & (i < S + 1))
        def _():
            forward_on(1, then(i - 1))

        @pl.when(near_at(i - 2))
        def _():
            complete(0, then(i - 2))
            project(then(i - 2))

        @pl.when((i >= 3) & (i < S + 2))
        def _():
            complete(1, then(i - 2))
            gradients(i - 2, then(i - 2))

        @pl.when((i >= 4) & (i < S + 3))
        def _():
            reduce_chip(i - 3, then(i - 3))

        @pl.when(i >= 6)
        def _():
            reduce_all(i - 5, then(i - 5))

        for j in range(2, SH):

            @pl.when(i == S // 2 + 1 + (S // 2) * (j - 1) // (SH - 1))
            def _():
                mix_step(j)

    each(1, S + 5, second)
    keep.start()
    keep_mix.start()

    tile = min(512, Q)
    per = Q // tile

    def weight_grads(i):
        q, c = lax.div(i, per), pl.multiple_of(lax.rem(i, per) * tile, tile)
        x = rows[0, :, q, :, pl.ds(c, tile)].reshape(S * cap, tile)
        start = pl.multiple_of(q * Q + c, tile)
        gout[pl.ds(start, tile), :] = dot(x, ggu[...].reshape(S * cap, 2 * H), TN).astype(jnp.bfloat16)
        d = rows[1, :, q, :, pl.ds(c, tile)].reshape(S * cap, tile)
        gdown[:, pl.ds(start, tile)] = dot(hid[...].reshape(S * cap, H), d, TN).astype(jnp.bfloat16)

    each(0, T * per, weight_grads)
    results = [
        pltpu.make_async_copy(gout.at[:, pl.ds(0, H)], gwg_h, gsem.at[0]),
        pltpu.make_async_copy(gout.at[:, pl.ds(H, H)], gwu_h, gsem.at[1]),
        pltpu.make_async_copy(gdown, gwd_h, gsem.at[2]),
    ]
    for copy in results:
        copy.start()

    half(S - 2).wait_send()
    half(S - 1).wait_send()

    def finish(k):
        for a in range(2):
            direct(a, k).wait_send()
            to_mate(a, k).wait_send()
            for j in range(1, TH):
                across(a, j, k).wait_send()
                on_to_mate(a, j, k).wait_send()
        give_back(k).wait_send()
        give_back(k).wait_recv()

    each(1, S, finish)

    def finish_sums(k):
        for j in range(1, TH):
            chip_sum(j, k).wait_send()

    each(0, S, finish_sums)
    keep.wait()
    mix_finish()
    for copy in results:
        copy.wait()


def mixer_kernel(
    S, T, placed, cot, out_gate, conv_out, in_gate, conv_in, taps, back_h, mix_h, w_out_h,
    gwo, gci, gig, gog,
    back, mix, w_out, total, res, colst, near, cols, conv, after,
    lsem, ds, dr, m1s, m1r, xs, xr, m2s, m2r, bs, br,
):
    TH = T // 2
    cap, Q = back.shape[1], back.shape[2]
    tok = cot.shape[0]
    piece, group = Q // S, T * Q // S
    s, t, th, tl = spot()
    mate = 2 * th + 1 - tl
    local = [
        pltpu.make_async_copy(src, dst, lsem.at[n])
        for n, (src, dst) in enumerate(((back_h, back), (mix_h, mix), (w_out_h, w_out)))
    ]
    for copy in local:
        copy.start()
    greet(S, TH)

    def other(j):
        return lax.rem(th + j, TH)

    def behind(j):
        return lax.rem(th - j + TH, TH)

    def at(i):
        return partner(S, s, i)

    def direct(k):
        peer = flip(S, s, k)
        return remote(colst.at[peer], cols.at[s, t], ds.at[k], dr.at[k], (peer, t))

    def direct_too(j, k):
        peer = flip(S, s, k)
        land = cols.at[s, 2 * other(j) + tl]
        return remote(near.at[j, k], land, xs.at[j, k], xr.at[TH - j, k], (peer, t))

    def block(k, q):
        return cols.at[flip(S, s, k), q] if k is not None else res.at[q]

    def to_mate(k):
        n = S if k is None else k
        return remote(block(k, t), block(k, t), m1s.at[n], m1r.at[n], (s, mate))

    def across(j, k):
        n = S if k is None else k
        return remote(block(k, t), block(k, t), xs.at[j, n], xr.at[j, n], (s, 2 * other(j) + tl))

    def on_to_mate(j, k):
        n = S if k is None else k
        q = 2 * behind(j) + tl
        return remote(block(k, q), block(k, q), m2s.at[j, n], m2r.at[j, n], (s, mate))

    def forward(k):
        @pl.when((S if k is None else k) >= NEAR)
        def _():
            for j in range(1, TH):
                across(j, k).start()

        to_mate(k).start()

    def forward_on(k):
        for j in range(1, TH):
            across(j, k).wait_recv()
            on_to_mate(j, k).start()

    def complete(k):
        to_mate(k).wait_recv()
        for j in range(1, TH):
            on_to_mate(j, k).wait_recv()

    def sent(k):
        to_mate(k).wait_send()
        for j in range(1, TH):
            across(j, k).wait_send()
            on_to_mate(j, k).wait_send()

    local[0].wait()
    total[...] = dot(placed[...].reshape(S * cap, tok), back[...].reshape(S * cap, Q), TN)
    for q in range(T):

        @pl.when(t == q)
        def _():
            for g in range(S):
                columns = pl.ds(g * piece, piece)
                mine = cot[:, pl.ds(g * group + q * piece, piece)].astype(jnp.float32)
                value = (mine + total[:, columns]).astype(jnp.bfloat16)
                res[q, :, columns] = value
                colst[g] = value

    forward(None)
    each(1, S, lambda i: direct(at(i)).start())

    def arrive(i):
        direct(at(i)).wait_recv()
        forward(at(i))

    local[2].wait()
    forward_on(None)
    each(1, S, arrive)
    complete(None)
    for g in range(S):

        @pl.when(s == g)
        def _():
            for q in range(T):
                cols[s, q] = res[q, :, pl.ds(g * piece, piece)]

        for k in range(1, min(NEAR, S)):

            @pl.when(flip(S, s, k) == g)
            def _():
                for j in range(1, TH):
                    near[j, k] = res[2 * other(j) + tl, :, pl.ds(g * piece, piece)]
                    direct_too(j, k).start()

    grad_mixed = jnp.zeros((tok, w_out.shape[1]), jnp.float32)
    for g in range(S):
        some = jnp.concatenate([res[q, :, pl.ds(g * piece, piece)] for q in range(T)], axis=1)
        grad_mixed = grad_mixed + dot(some, w_out[pl.ds(g * group, group), :])
    gog[...] = (grad_mixed * conv_out[...].astype(jnp.float32)).astype(jnp.bfloat16)
    conv[pl.ds(0, tok), :] = grad_mixed * out_gate[...].astype(jnp.float32)

    def edge(target):
        return remote(conv.at[pl.ds(0, 8), :], after, bs.at[0], br.at[0], (target, t))

    @pl.when(s > 0)
    def _():
        edge(s - 1).start()

    local[1].wait()

    def take(k):
        @pl.when(k > 0)
        def _():
            complete(k)
        b = flip(S, s, k)
        columns = jnp.concatenate([cols[b, q] for q in range(T)], axis=1)
        gwo[...] += dot(columns, mix[b], TN)

    gwo[...] = jnp.zeros_like(gwo)
    take(0)

    def turn(i):
        return at(jnp.where(i <= S - NEAR, i + NEAR - 1, i - (S - NEAR)))

    def step(i):
        @pl.when(i < S)
        def _():
            forward_on(turn(i))

        @pl.when(i >= 2)
        def _():
            take(turn(i - 1))

    each(1, S + 1, step)

    @pl.when(s < S - 1)
    def _():
        edge(0).wait_recv()
        conv[pl.ds(tok, 8), :] = after[...]

    @pl.when(s == S - 1)
    def _():
        conv[pl.ds(tok, 8), :] = jnp.zeros_like(after)

    grad_g = (
        taps[2:3, :] * conv[pl.ds(0, tok), :]
        + taps[1:2, :] * conv[pl.ds(1, tok), :]
        + taps[0:1, :] * conv[pl.ds(2, tok), :]
    )
    gci[...] = (grad_g * in_gate[...].astype(jnp.float32)).astype(jnp.bfloat16)
    gig[...] = (grad_g * conv_in[...].astype(jnp.float32)).astype(jnp.bfloat16)

    @pl.when(s > 0)
    def _():
        edge(s - 1).wait_send()

    sent(None)
    each(1, S, sent)
    each(1, S, lambda k: direct(k).wait_send())


def expert_exchange(S, T, cap, inp, cot, placed, slot_w, out_gate, conv_out, w_gate, w_up, w_down):
    tok, D = inp.shape
    H = w_down.shape[0]
    TH, Q, SH = T // 2, D // T, S // 2
    bf, f32 = jnp.bfloat16, jnp.float32
    dma = pltpu.SemaphoreType.DMA
    vmem = pl.BlockSpec(memory_space=pltpu.VMEM)
    hbm = pl.BlockSpec(memory_space=pl.ANY)
    rows = S * cap
    return pl.pallas_call(
        functools.partial(expert_kernel, S, T),
        name="expert_exchange",
        out_shape=(
            jax.ShapeDtypeStruct((S, cap, Q), bf),
            jax.ShapeDtypeStruct((S,) + out_gate.shape, bf),
            jax.ShapeDtypeStruct((D, H), bf),
            jax.ShapeDtypeStruct((D, H), bf),
            jax.ShapeDtypeStruct((H, D), bf),
        ),
        in_specs=[vmem] * 6 + [hbm] * 3,
        out_specs=(hbm,) * 5,
        scratch_shapes=[
            pltpu.VMEM(out_gate.shape, bf),
            pltpu.VMEM((2, S, T, cap, Q), bf),
            pltpu.VMEM((2, S, cap, Q), bf),
            pltpu.VMEM((D, 2 * H), bf),
            pltpu.VMEM((H, D), bf),
            pltpu.VMEM((S, cap, 2 * H), f32),
            pltpu.VMEM((S, cap, H), bf),
            pltpu.VMEM((S, cap, 2 * H), bf),
            pltpu.VMEM((2, 2, TH, cap, Q), f32),
            pltpu.VMEM((S, TH, cap, Q), f32),
            pltpu.VMEM((3, cap, Q), f32),
            pltpu.VMEM((2, TH, NEAR, cap, Q), bf),
            pltpu.VMEM((TH, S, cap, Q), bf),
            pltpu.VMEM((TH, S, cap, Q), bf),
            pltpu.VMEM((S, cap, Q), bf),
            pltpu.VMEM((D, 2 * H), bf),
            pltpu.VMEM((H, D), bf),
            dma((3,)), dma((4,)),
            dma((2, S)), dma((2, S)),
            dma((2, S)), dma((2, S)),
            dma((2, TH, S)), dma((2, TH, S)),
            dma((2, TH, S)), dma((2, TH, S)),
            dma((S,)), dma((S,)),
            dma((TH, S)), dma((TH, S)),
            dma((S,)), dma((S,)),
            dma((SH,)), dma((SH + 1,)),
            dma((SH,)), dma((SH + 1,)),
            dma((SH,)), dma((SH,)),
        ],
        cost_estimate=pl.CostEstimate(
            flops=16 * rows * D * H, bytes_accessed=8 * rows * D + 24 * D * H, transcendentals=rows * H
        ),
        compiler_params=pltpu.CompilerParams(
            collective_id=0, has_side_effects=True, vmem_limit_bytes=67_043_328
        ),
    )(inp, cot, placed, slot_w, out_gate, conv_out, w_gate, w_up, w_down)


def mixer(S, T, placed, cot, out_gate, conv_out, in_gate, conv_in, taps, back, mix_all, w_out):
    tok, D = cot.shape
    B = w_out.shape[1]
    cap = placed.shape[1]
    TH, Q = T // 2, D // T
    bf, f32 = jnp.bfloat16, jnp.float32
    dma = pltpu.SemaphoreType.DMA
    vmem = pl.BlockSpec(memory_space=pltpu.VMEM)
    hbm = pl.BlockSpec(memory_space=pl.ANY)
    small = jax.ShapeDtypeStruct((tok, B), bf)
    return pl.pallas_call(
        functools.partial(mixer_kernel, S, T),
        name="mixer",
        out_shape=(jax.ShapeDtypeStruct((D // S, B), f32), small, small, small),
        in_specs=[vmem] * 7 + [hbm] * 3,
        out_specs=(vmem,) * 4,
        scratch_shapes=[
            pltpu.VMEM((S, cap, Q), bf),
            pltpu.VMEM((S, tok, B), bf),
            pltpu.VMEM((D, B), bf),
            pltpu.VMEM((tok, Q), f32),
            pltpu.VMEM((T, tok, Q), bf),
            pltpu.VMEM((S, tok, Q // S), bf),
            pltpu.VMEM((TH, NEAR, tok, Q // S), bf),
            pltpu.VMEM((S, T, tok, Q // S), bf),
            pltpu.VMEM((tok + 8, B), f32),
            pltpu.VMEM((8, B), f32),
            dma((3,)),
            dma((S,)), dma((S,)),
            dma((S + 1,)), dma((S + 1,)),
            dma((TH, S + 1)), dma((TH, S + 1)),
            dma((TH, S + 1)), dma((TH, S + 1)),
            dma((1,)), dma((1,)),
        ],
        cost_estimate=pl.CostEstimate(
            flops=2 * tok * D * B * 2 + 2 * S * cap * tok * Q, bytes_accessed=4 * D * B, transcendentals=0
        ),
        compiler_params=pltpu.CompilerParams(
            collective_id=1, has_side_effects=True, vmem_limit_bytes=67_043_328
        ),
    )(placed, cot, out_gate, conv_out, in_gate, conv_in, taps, back, mix_all, w_out)


def slot_masks(routes, route_weight, experts, capacity):
    tok_rows = routes.shape[0]
    names = jnp.arange(experts, dtype=jnp.int32)
    hits = routes[None, :, :] == names[:, None, None]
    chosen = jnp.any(hits, axis=2)
    weight = jnp.sum(jnp.where(hits, route_weight[None], 0.0), axis=2)
    order = jnp.arange(tok_rows, dtype=jnp.int32)
    before = (order[:, None] < order[None, :]).astype(jnp.bfloat16)
    rank = jnp.dot(chosen.astype(jnp.bfloat16), before, preferred_element_type=jnp.float32)
    rank = jnp.where(chosen, rank.astype(jnp.int32), -1)
    slots = jnp.arange(capacity, dtype=jnp.int32)
    placed = rank[:, None, :] == slots[None, :, None]
    slot_weight = jnp.sum(jnp.where(placed, weight[:, None, :], 0.0), axis=2, keepdims=True)
    return placed.astype(jnp.bfloat16), slot_weight


def per_device(
    cotangent, moe_input, routes, route_weight, conv_input, input_gate, output_gate, conv_output,
    taps, w_out, w_gate, w_up, w_down,
):
    experts = lax.axis_size("sp")
    tp_size = lax.axis_size("tp")
    tok_rows, top_k = routes.shape
    capacity = -(-max(2, 2 * tok_rows * top_k // experts) // 16) * 16
    placed, slot_weight = slot_masks(routes, route_weight, experts, capacity)
    returned, mixed_all, gate_wgrad, up_wgrad, grad_down = expert_exchange(
        experts, tp_size, capacity, moe_input, cotangent, placed, slot_weight, output_gate, conv_output,
        w_gate[0], w_up[0], w_down[0],
    )
    grad_w_out, grad_conv_input, grad_input_gate, grad_output_gate = mixer(
        experts, tp_size, placed, cotangent, output_gate, conv_output, input_gate, conv_input, taps,
        returned, mixed_all, w_out,
    )
    return (
        gate_wgrad[None], up_wgrad[None], grad_down[None], grad_w_out,
        grad_conv_input, grad_input_gate, grad_output_gate,
    )


def solution(mesh):
    return jax.shard_map(
        per_device,
        mesh=mesh,
        in_specs=(
            P("sp", None), P("sp", None), P("sp", None), P("sp", None),
            P("sp", "tp"), P("sp", "tp"), P("sp", "tp"), P("sp", "tp"),
            P(None, "tp"), P(None, "tp"),
            P("sp", None, "tp"), P("sp", None, "tp"), P("sp", "tp", None),
        ),
        out_specs=(
            P("sp", None, "tp"), P("sp", None, "tp"), P("sp", "tp", None),
            P("sp", "tp"), P("sp", "tp"), P("sp", "tp"), P("sp", "tp"),
        ),
        check_vma=False,
    )
```

```python
import functools

import jax
import jax.numpy as jnp
from jax import lax
from jax.experimental import pallas as pl
from jax.experimental.pallas import tpu as pltpu
from jax.sharding import PartitionSpec as P

NEAR = 4
CUTS = 4
MESH = pl.DeviceIdType.MESH
NN = (((1,), (0,)), ((), ()))
NT = (((1,), (1,)), ((), ()))
TN = (((0,), (0,)), ((), ()))


def dot(a, b, dims=NN):
    return lax.dot_general(a, b, dims, preferred_element_type=jnp.float32)


def each(low, high, step):
    def body(i, carry):
        step(i)
        return carry

    lax.fori_loop(low, high, body, 0)


def spot():
    s, t = lax.axis_index("sp"), lax.axis_index("tp")
    return s, t, lax.div(t, 2), lax.rem(t, 2)


def flip(S, a, b):
    total, weight = 0, 1
    while weight < S:
        p, q = lax.rem(lax.div(a, weight), 2), lax.rem(lax.div(b, weight), 2)
        total, weight = total + (p + q - 2 * p * q) * weight, 2 * weight
    return total


def partner(S, s, i):
    if S < 4:
        return i
    high, low = lax.div(s, S // 2), lax.rem(lax.div(s, S // 4), 2)
    inner = high + low - 2 * high * low
    turned = S // 2 + lax.rem(i - S // 2 + inner * (S // 4) + S, S // 2)
    return jnp.where(i >= S // 2, turned, i)


def remote(src, dst, send, recv, device):
    return pltpu.make_async_remote_copy(
        src_ref=src, dst_ref=dst, send_sem=send, recv_sem=recv, device_id=device, device_id_type=MESH
    )


def greet(S, TH):
    s, t, th, tl = spot()
    barrier = pltpu.get_barrier_semaphore()

    def hello(device):
        pl.semaphore_signal(barrier, inc=1, device_id=device, device_id_type=MESH)

    each(1, S, lambda k: hello((lax.rem(s + k, S), t)))
    hello((s, 2 * th + 1 - tl))
    for j in range(1, TH):
        hello((s, 2 * lax.rem(th + j, TH) + tl))
    pl.semaphore_wait(barrier, S - 1 + TH)


def expert_kernel(
    S, T, inp, cot, placed, weight, out_gate, conv_out, wg_h, wu_h, wd_h,
    back, mix_all, gwg_h, gwu_h, gwd_h,
    mix, rows, stage, wgu, wd, proj, hid, ggu, part, matebuf, total_part, near, xsend, xrecv, rstage, gout, gdown,
    wsem, gsem, ds, dr, m1s, m1r, xs, xr, m2s, m2r, r1s, r1r, r2s, r2r, rts, rtr, us, ur, vs, vr, ys, yr,
):
    TH = T // 2
    cap, Q = rows.shape[3], rows.shape[4]
    D = T * Q
    H = wd.shape[0]
    piece = Q // S
    group = D // S
    s, t, th, tl = spot()
    mate = 2 * th + 1 - tl
    source = (inp, cot)

    def other(j):
        return lax.rem(th + j, TH)

    def behind(j):
        return lax.rem(th - j + TH, TH)

    def src_of(k):
        return flip(S, s, k)

    def at(i):
        return partner(S, s, i)

    weights = [
        pltpu.make_async_copy(wg_h, wgu.at[:, pl.ds(0, H)], wsem.at[0]),
        pltpu.make_async_copy(wu_h, wgu.at[:, pl.ds(H, H)], wsem.at[1]),
        pltpu.make_async_copy(wd_h, wd, wsem.at[2]),
    ]
    for copy in weights:
        copy.start()
    greet(S, TH)

    def direct(a, k):
        return remote(stage.at[a, k], rows.at[a, s, t], ds.at[a, k], dr.at[a, k], (src_of(k), t))

    def direct_too(a, j, k):
        q = 2 * other(j) + tl
        return remote(near.at[a, j, k], rows.at[a, s, q], xs.at[a, j, k], xr.at[a, TH - j, k], (src_of(k), t))

    def to_mate(a, k):
        block = rows.at[a, src_of(k), t]
        return remote(block, block, m1s.at[a, k], m1r.at[a, k], (s, mate))

    def across(a, j, k):
        block = rows.at[a, src_of(k), t]
        return remote(block, block, xs.at[a, j, k], xr.at[a, j, k], (s, 2 * other(j) + tl))

    def on_to_mate(a, j, k):
        block = rows.at[a, src_of(k), 2 * behind(j) + tl]
        return remote(block, block, m2s.at[a, j, k], m2r.at[a, j, k], (s, mate))

    def pick(a, e, columns):
        picked = dot(placed[e], source[a][:, columns])
        if a == 1:
            picked = picked * jnp.sum(placed[e].astype(jnp.float32) * weight[pl.ds(e, 1), :], axis=1, keepdims=True)
        return picked.astype(jnp.bfloat16)

    def send(a, k):
        stage[a, k] = pick(a, src_of(k), pl.ds(pl.multiple_of(t * Q, Q), Q))
        direct(a, k).start()

        @pl.when(k < NEAR)
        def _():
            for j in range(1, TH):
                near[a, j, k] = pick(a, src_of(k), pl.ds(pl.multiple_of((2 * other(j) + tl) * Q, Q), Q))
                direct_too(a, j, k).start()

    def own(a):
        for q in range(T):
            rows[a, s, q] = pick(a, s, pl.ds(q * Q, Q))

    def forward(a, k):
        direct(a, k).wait_recv()

        @pl.when(k >= NEAR)
        def _():
            for j in range(1, TH):
                across(a, j, k).start()

        to_mate(a, k).start()

    def forward_on(a, k):
        for j in range(1, TH):
            across(a, j, k).wait_recv()
            on_to_mate(a, j, k).start()

    def complete(a, k):
        to_mate(a, k).wait_recv()
        for j in range(1, TH):
            on_to_mate(a, j, k).wait_recv()

    def project(k):
        b = src_of(k)
        total = dot(rows[0, b, 0], wgu[pl.ds(0, Q), :])
        for q in range(1, T):
            total = total + dot(rows[0, b, q], wgu[pl.ds(q * Q, Q), :])
        proj[b] = total

    def half(n):
        return remote(part.at[lax.rem(n, 2), 1 - tl], matebuf.at[n], r1s.at[n], r1r.at[n], (s, mate))

    def chip_sum(j, k):
        return remote(xsend.at[j, k], xrecv.at[j, k], r2s.at[j, k], r2r.at[j, k], (s, 2 * other(j) + tl))

    def give_back(k):
        return remote(rstage.at[k], back.at[s], rts.at[k], rtr.at[k], (src_of(k), t))

    def gradients(n, k):
        b = src_of(k)
        grad_hidden = dot(rows[1, b, 0], wd[:, pl.ds(0, Q)], NT)
        for q in range(1, T):
            grad_hidden = grad_hidden + dot(rows[1, b, q], wd[:, pl.ds(q * Q, Q)], NT)
        gate, up = proj[b][:, :H], proj[b][:, H:]
        sig = jax.nn.sigmoid(gate)
        act = gate * sig
        slope = sig * (1.0 + gate * (1.0 - sig))
        hid[b] = (act * up).astype(jnp.bfloat16)
        ggu[b, :, pl.ds(0, H)] = (grad_hidden * up * slope).astype(jnp.bfloat16)
        ggu[b, :, pl.ds(H, H)] = (grad_hidden * act).astype(jnp.bfloat16)

        @pl.when(n >= 2)
        def _():
            half(n - 2).wait_send()

        slot = lax.rem(n, 2)
        grads = ggu[b]
        for g in range(S):
            some = dot(grads, wgu[pl.ds(g * group, group), :], NT)
            for q in range(T):
                part[slot, q % 2, q // 2, :, pl.ds(g * piece, piece)] = some[:, q * piece : (q + 1) * piece]
        half(n).start()

    def reduce_chip(n, k):
        half(n).wait_recv()
        slot = lax.rem(n, 2)
        for j in range(1, TH):
            o = other(j)
            xsend[j, k] = (part[slot, tl, o] + matebuf[n, o]).astype(jnp.bfloat16)
            chip_sum(j, k).start()
        total_part[lax.rem(n, 3)] = part[slot, tl, th] + matebuf[n, th]

    def reduce_all(n, k):
        total = total_part[lax.rem(n, 3)]
        for j in range(1, TH):
            chip_sum(j, k).wait_recv()
            total = total + xrecv[j, k].astype(jnp.float32)
        rstage[k] = total.astype(jnp.bfloat16)

        @pl.when(k >= 1)
        def _():
            give_back(k).start()

    SH = S // 2
    sh, sl = lax.div(s, 2), lax.rem(s, 2)

    def block(h):
        return mix_all.at[2 * h + sl]

    def rise(j):
        return remote(mix if j == 0 else block(sh - j), block(sh - j), us.at[j], ur.at[j + 1], (s + 2, t))

    def sink(j):
        return remote(mix if j == 0 else block(sh + j), block(sh + j), vs.at[j], vr.at[j + 1], (s - 2, t))

    def side(h, value=None):
        return remote(block(h) if value is None else value, block(h), ys.at[h], yr.at[h], (2 * sh + 1 - sl, t))

    def mix_step(j):
        if j == 0:
            side(sh, mix).start()

            @pl.when(sh < SH - 1)
            def _():
                rise(0).start()

            @pl.when(sh > 0)
            def _():
                sink(0).start()

            return

        @pl.when(sh >= j)
        def _():
            remote(block(sh - j), block(sh - j), us.at[j], ur.at[j], (s, mate)).wait_recv()

            @pl.when(sh < SH - 1)
            def _():
                rise(j).start()

            side(sh - j).start()

        @pl.when(sh + j < SH)
        def _():
            remote(block(sh + j), block(sh + j), vs.at[j], vr.at[j], (s, mate)).wait_recv()

            @pl.when(sh > 0)
            def _():
                sink(j).start()

            side(sh + j).start()

    def mix_finish():
        keep_mix.wait()
        for j in range(SH - 1):

            @pl.when((sh >= j) & (sh < SH - 1))
            def _():
                rise(j).wait_send()

            @pl.when((sh + j < SH) & (sh > 0))
            def _():
                sink(j).wait_send()

        def one(h):
            side(h).wait_send()
            side(h).wait_recv()

        each(0, SH, one)

    keep_mix = pltpu.make_async_copy(mix, mix_all.at[s], gsem.at[3])
    keep = pltpu.make_async_copy(rstage.at[0], back.at[s], rts.at[0])

    mix[...] = (out_gate[...].astype(jnp.float32) * conv_out[...].astype(jnp.float32)).astype(jnp.bfloat16)
    middle = max(2, S // 2)
    each(middle, S, lambda i: send(0, at(i)))
    mix_step(0)
    each(1, middle, lambda i: send(0, at(i)))
    each(1, middle, lambda i: send(1, at(i)))
    own(0)
    own(1)
    for copy in weights:
        copy.wait()
    project(0)
    gradients(0, 0)

    def first(i):
        @pl.when(i < S)
        def _():
            forward(0, at(i))

        @pl.when(i == S - 1)
        def _():
            each(middle, S, lambda m: send(1, at(m)))

        @pl.when(i == middle + 1)
        def _():
            reduce_chip(0, 0)

        @pl.when(i == middle + 3)
        def _():
            reduce_all(0, 0)

        @pl.when((i >= middle + 1) & (i < S + 1))
        def _():
            forward_on(0, at(i - 1))

        @pl.when(i >= middle + 2)
        def _():
            complete(0, at(i - 2))
            project(at(i - 2))

    each(middle, S + 2, first)
    mix_step(1)

    lead = S // 4

    def near_at(i):
        return (i > lead) & (i < lead + middle)

    def then(i):
        return jnp.where(i <= lead, at(i + middle - 1), jnp.where(i < lead + middle, at(i - lead), at(i)))

    def second(i):
        @pl.when(near_at(i))
        def _():
            forward(0, then(i))

        @pl.when(i < S)
        def _():
            forward(1, then(i))

        @pl.when(near_at(i - 1))
        def _():
            forward_on(0, then(i - 1))

        @pl.when((i >= 2) & (i < S + 1))
        def _():
            forward_on(1, then(i - 1))

        @pl.when(near_at(i - 2))
        def _():
            complete(0, then(i - 2))
            project(then(i - 2))

        @pl.when((i >= 3) & (i < S + 2))
        def _():
            complete(1, then(i - 2))
            gradients(i - 2, then(i - 2))

        @pl.when((i >= 4) & (i < S + 3))
        def _():
            reduce_chip(i - 3, then(i - 3))

        @pl.when(i >= 6)
        def _():
            reduce_all(i - 5, then(i - 5))

        for j in range(2, SH):

            @pl.when(i == S // 2 + 1 + (S // 2) * (j - 1) // (SH - 1))
            def _():
                mix_step(j)

    each(1, S + 5, second)
    keep.start()
    keep_mix.start()

    tile = min(512, Q)
    per = Q // tile

    def weight_grads(i):
        q, c = lax.div(i, per), pl.multiple_of(lax.rem(i, per) * tile, tile)
        x = rows[0, :, q, :, pl.ds(c, tile)].reshape(S * cap, tile)
        start = pl.multiple_of(q * Q + c, tile)
        gout[pl.ds(start, tile), :] = dot(x, ggu[...].reshape(S * cap, 2 * H), TN).astype(jnp.bfloat16)
        d = rows[1, :, q, :, pl.ds(c, tile)].reshape(S * cap, tile)
        gdown[:, pl.ds(start, tile)] = dot(hid[...].reshape(S * cap, H), d, TN).astype(jnp.bfloat16)

    each(0, T * per, weight_grads)
    results = [
        pltpu.make_async_copy(gout.at[:, pl.ds(0, H)], gwg_h, gsem.at[0]),
        pltpu.make_async_copy(gout.at[:, pl.ds(H, H)], gwu_h, gsem.at[1]),
        pltpu.make_async_copy(gdown, gwd_h, gsem.at[2]),
    ]
    for copy in results:
        copy.start()

    half(S - 2).wait_send()
    half(S - 1).wait_send()

    def finish(k):
        for a in range(2):
            direct(a, k).wait_send()
            to_mate(a, k).wait_send()
            for j in range(1, TH):
                across(a, j, k).wait_send()
                on_to_mate(a, j, k).wait_send()
        give_back(k).wait_send()
        give_back(k).wait_recv()

    each(1, S, finish)

    def finish_sums(k):
        for j in range(1, TH):
            chip_sum(j, k).wait_send()

    each(0, S, finish_sums)
    keep.wait()
    mix_finish()
    for copy in results:
        copy.wait()


def mixer_kernel(
    S, T, placed, cot, out_gate, back_h, mix_h, w_out_h,
    gwo, gm, shifted,
    back, mix, w_out, total, res, colst, near, cols, conv, after,
    lsem, ds, dr, m1s, m1r, xs, xr, m2s, m2r, bs, br,
):
    TH = T // 2
    cap, Q = back.shape[1], back.shape[2]
    tok = cot.shape[0]
    piece, group = Q // S, T * Q // S
    s, t, th, tl = spot()
    mate = 2 * th + 1 - tl
    local = [
        pltpu.make_async_copy(src, dst, lsem.at[n])
        for n, (src, dst) in enumerate(((back_h, back), (mix_h, mix), (w_out_h, w_out)))
    ]
    for copy in local:
        copy.start()
    greet(S, TH)

    def other(j):
        return lax.rem(th + j, TH)

    def behind(j):
        return lax.rem(th - j + TH, TH)

    def at(i):
        return partner(S, s, i)

    def direct(k):
        peer = flip(S, s, k)
        return remote(colst.at[peer], cols.at[s, t], ds.at[k], dr.at[k], (peer, t))

    def direct_too(j, k):
        peer = flip(S, s, k)
        land = cols.at[s, 2 * other(j) + tl]
        return remote(near.at[j, k], land, xs.at[j, k], xr.at[TH - j, k], (peer, t))

    def block(k, q):
        return cols.at[flip(S, s, k), q] if k is not None else res.at[q]

    def to_mate(k):
        n = S if k is None else k
        return remote(block(k, t), block(k, t), m1s.at[n], m1r.at[n], (s, mate))

    def across(j, k):
        n = S if k is None else k
        return remote(block(k, t), block(k, t), xs.at[j, n], xr.at[j, n], (s, 2 * other(j) + tl))

    def on_to_mate(j, k):
        n = S if k is None else k
        q = 2 * behind(j) + tl
        return remote(block(k, q), block(k, q), m2s.at[j, n], m2r.at[j, n], (s, mate))

    def forward(k):
        @pl.when((S if k is None else k) >= NEAR)
        def _():
            for j in range(1, TH):
                across(j, k).start()

        to_mate(k).start()

    def forward_on(k):
        for j in range(1, TH):
            across(j, k).wait_recv()
            on_to_mate(j, k).start()

    def complete(k):
        to_mate(k).wait_recv()
        for j in range(1, TH):
            on_to_mate(j, k).wait_recv()

    def sent(k):
        to_mate(k).wait_send()
        for j in range(1, TH):
            across(j, k).wait_send()
            on_to_mate(j, k).wait_send()

    local[0].wait()
    total[...] = dot(placed[...].reshape(S * cap, tok), back[...].reshape(S * cap, Q), TN)
    for q in range(T):

        @pl.when(t == q)
        def _():
            for g in range(S):
                columns = pl.ds(g * piece, piece)
                mine = cot[:, pl.ds(g * group + q * piece, piece)].astype(jnp.float32)
                value = (mine + total[:, columns]).astype(jnp.bfloat16)
                res[q, :, columns] = value
                colst[g] = value

    forward(None)
    each(1, S, lambda i: direct(at(i)).start())

    def arrive(i):
        direct(at(i)).wait_recv()
        forward(at(i))

    local[2].wait()
    forward_on(None)
    each(1, S, arrive)
    complete(None)
    for g in range(S):

        @pl.when(s == g)
        def _():
            for q in range(T):
                cols[s, q] = res[q, :, pl.ds(g * piece, piece)]

        for k in range(1, min(NEAR, S)):

            @pl.when(flip(S, s, k) == g)
            def _():
                for j in range(1, TH):
                    near[j, k] = res[2 * other(j) + tl, :, pl.ds(g * piece, piece)]
                    direct_too(j, k).start()

    grad_mixed = jnp.zeros((tok, w_out.shape[1]), jnp.float32)
    for g in range(S):
        some = jnp.concatenate([res[q, :, pl.ds(g * piece, piece)] for q in range(T)], axis=1)
        grad_mixed = grad_mixed + dot(some, w_out[pl.ds(g * group, group), :])
    gm[...] = grad_mixed
    conv[pl.ds(0, tok), :] = grad_mixed * out_gate[...].astype(jnp.float32)

    def edge(target):
        return remote(conv.at[pl.ds(0, 8), :], after, bs.at[0], br.at[0], (target, t))

    @pl.when(s > 0)
    def _():
        edge(s - 1).start()

    local[1].wait()

    def take(k):
        @pl.when(k > 0)
        def _():
            complete(k)
        b = flip(S, s, k)
        columns = jnp.concatenate([cols[b, q] for q in range(T)], axis=1)
        gwo[...] += dot(columns, mix[b], TN)

    gwo[...] = jnp.zeros_like(gwo)
    take(0)

    def turn(i):
        return at(jnp.where(i <= S - NEAR, i + NEAR - 1, i - (S - NEAR)))

    def step(i):
        @pl.when(i < S)
        def _():
            forward_on(turn(i))

        @pl.when(i >= 2)
        def _():
            take(turn(i - 1))

    each(1, S + 1, step)

    @pl.when(s < S - 1)
    def _():
        edge(0).wait_recv()
        conv[pl.ds(tok, 8), :] = after[...]

    @pl.when(s == S - 1)
    def _():
        conv[pl.ds(tok, 8), :] = jnp.zeros_like(after)

    shifted[...] = conv[...]

    @pl.when(s > 0)
    def _():
        edge(s - 1).wait_send()

    sent(None)
    each(1, S, sent)
    each(1, S, lambda k: direct(k).wait_send())


def expert_exchange(S, T, cap, inp, cot, placed, weight, out_gate, conv_out, w_gate, w_up, w_down):
    tok, D = inp.shape
    H = w_down.shape[0]
    TH, Q, SH = T // 2, D // T, S // 2
    bf, f32 = jnp.bfloat16, jnp.float32
    dma = pltpu.SemaphoreType.DMA
    vmem = pl.BlockSpec(memory_space=pltpu.VMEM)
    hbm = pl.BlockSpec(memory_space=pl.ANY)
    rows = S * cap
    return pl.pallas_call(
        functools.partial(expert_kernel, S, T),
        name="expert_exchange",
        out_shape=(
            jax.ShapeDtypeStruct((S, cap, Q), bf),
            jax.ShapeDtypeStruct((S,) + out_gate.shape, bf),
            jax.ShapeDtypeStruct((D, H), bf),
            jax.ShapeDtypeStruct((D, H), bf),
            jax.ShapeDtypeStruct((H, D), bf),
        ),
        in_specs=[vmem] * 6 + [hbm] * 3,
        out_specs=(hbm,) * 5,
        scratch_shapes=[
            pltpu.VMEM(out_gate.shape, bf),
            pltpu.VMEM((2, S, T, cap, Q), bf),
            pltpu.VMEM((2, S, cap, Q), bf),
            pltpu.VMEM((D, 2 * H), bf),
            pltpu.VMEM((H, D), bf),
            pltpu.VMEM((S, cap, 2 * H), f32),
            pltpu.VMEM((S, cap, H), bf),
            pltpu.VMEM((S, cap, 2 * H), bf),
            pltpu.VMEM((2, 2, TH, cap, Q), f32),
            pltpu.VMEM((S, TH, cap, Q), f32),
            pltpu.VMEM((3, cap, Q), f32),
            pltpu.VMEM((2, TH, NEAR, cap, Q), bf),
            pltpu.VMEM((TH, S, cap, Q), bf),
            pltpu.VMEM((TH, S, cap, Q), bf),
            pltpu.VMEM((S, cap, Q), bf),
            pltpu.VMEM((D, 2 * H), bf),
            pltpu.VMEM((H, D), bf),
            dma((3,)), dma((4,)),
            dma((2, S)), dma((2, S)),
            dma((2, S)), dma((2, S)),
            dma((2, TH, S)), dma((2, TH, S)),
            dma((2, TH, S)), dma((2, TH, S)),
            dma((S,)), dma((S,)),
            dma((TH, S)), dma((TH, S)),
            dma((S,)), dma((S,)),
            dma((SH,)), dma((SH + 1,)),
            dma((SH,)), dma((SH + 1,)),
            dma((SH,)), dma((SH,)),
        ],
        cost_estimate=pl.CostEstimate(
            flops=16 * rows * D * H, bytes_accessed=8 * rows * D + 24 * D * H, transcendentals=rows * H
        ),
        compiler_params=pltpu.CompilerParams(
            collective_id=0, has_side_effects=True, vmem_limit_bytes=67_043_328
        ),
    )(inp, cot, placed, weight, out_gate, conv_out, w_gate, w_up, w_down)


def mixer(S, T, placed, cot, out_gate, back, mix_all, w_out):
    tok, D = cot.shape
    B = w_out.shape[1]
    cap = placed.shape[1]
    TH, Q = T // 2, D // T
    bf, f32 = jnp.bfloat16, jnp.float32
    dma = pltpu.SemaphoreType.DMA
    vmem = pl.BlockSpec(memory_space=pltpu.VMEM)
    hbm = pl.BlockSpec(memory_space=pl.ANY)
    return pl.pallas_call(
        functools.partial(mixer_kernel, S, T),
        name="mixer",
        out_shape=tuple(jax.ShapeDtypeStruct((n, B), f32) for n in (D // S, tok, tok + 8)),
        in_specs=[vmem] * 3 + [hbm] * 3,
        out_specs=(vmem,) * 3,
        scratch_shapes=[
            pltpu.VMEM((S, cap, Q), bf),
            pltpu.VMEM((S, tok, B), bf),
            pltpu.VMEM((D, B), bf),
            pltpu.VMEM((tok, Q), f32),
            pltpu.VMEM((T, tok, Q), bf),
            pltpu.VMEM((S, tok, Q // S), bf),
            pltpu.VMEM((TH, NEAR, tok, Q // S), bf),
            pltpu.VMEM((S, T, tok, Q // S), bf),
            pltpu.VMEM((tok + 8, B), f32),
            pltpu.VMEM((8, B), f32),
            dma((3,)),
            dma((S,)), dma((S,)),
            dma((S + 1,)), dma((S + 1,)),
            dma((TH, S + 1)), dma((TH, S + 1)),
            dma((TH, S + 1)), dma((TH, S + 1)),
            dma((1,)), dma((1,)),
        ],
        cost_estimate=pl.CostEstimate(
            flops=2 * tok * D * B * 2 + 2 * S * cap * tok * Q, bytes_accessed=4 * D * B, transcendentals=0
        ),
        compiler_params=pltpu.CompilerParams(
            collective_id=1, has_side_effects=True, vmem_limit_bytes=67_043_328
        ),
    )(placed, cot, out_gate, back, mix_all, w_out)


def finish_kernel(parts, gm, conv, conv_out, in_gate, conv_in, taps, *refs):
    n = len(parts)
    ins, gog, gci, gig, outs = refs[:n], refs[n], refs[n + 1], refs[n + 2], refs[n + 3 : 2 * n + 3]
    held, insem, outsem = refs[2 * n + 3 : 3 * n + 3], refs[3 * n + 3], refs[3 * n + 4]
    tok = gm.shape[0]
    pieces = []
    for m in range(n):
        rows = parts[m].shape[0] // CUTS
        for c in range(CUTS):
            cut, sem = pl.ds(c * rows, rows), m * CUTS + c
            take = pltpu.make_async_copy(ins[m].at[cut, :], held[m].at[cut, :], insem.at[sem])
            give = pltpu.make_async_copy(held[m].at[cut, :], outs[m].at[cut, :], outsem.at[sem])
            take.start()
            pieces.append((take, give))
    for take, give in pieces[: len(pieces) // 2]:
        take.wait()
        give.start()
    grad_g = (
        taps[2:3, :] * conv[pl.ds(0, tok), :]
        + taps[1:2, :] * conv[pl.ds(1, tok), :]
        + taps[0:1, :] * conv[pl.ds(2, tok), :]
    )
    gog[...] = (gm[...] * conv_out[...].astype(jnp.float32)).astype(jnp.bfloat16)
    gci[...] = (grad_g * in_gate[...].astype(jnp.float32)).astype(jnp.bfloat16)
    gig[...] = (grad_g * conv_in[...].astype(jnp.float32)).astype(jnp.bfloat16)
    for take, give in pieces[len(pieces) // 2 :]:
        take.wait()
        give.start()
    for _, give in pieces:
        give.wait()


def finish(gm, conv, conv_out, in_gate, conv_in, taps, *parts):
    vmem = pl.BlockSpec(memory_space=pltpu.VMEM)
    hbm = pl.BlockSpec(memory_space=pl.ANY)
    shapes = tuple(jax.ShapeDtypeStruct(part.shape, part.dtype) for part in parts)
    small = jax.ShapeDtypeStruct(conv_out.shape, conv_out.dtype)
    return pl.pallas_call(
        functools.partial(finish_kernel, shapes),
        name="finish",
        out_shape=(small, small, small) + shapes,
        in_specs=[vmem] * 6 + [hbm] * len(parts),
        out_specs=(vmem,) * 3 + (hbm,) * len(parts),
        scratch_shapes=[pltpu.VMEM(part.shape, part.dtype) for part in parts]
        + [pltpu.SemaphoreType.DMA((len(parts) * CUTS,))] * 2,
        compiler_params=pltpu.CompilerParams(vmem_limit_bytes=67_043_328),
    )(gm, conv, conv_out, in_gate, conv_in, taps, *parts)


def slot_masks(routes, route_weight, experts, capacity):
    tok_rows = routes.shape[0]
    names = jnp.arange(experts, dtype=jnp.int32)
    hits = routes[None, :, :] == names[:, None, None]
    chosen = jnp.any(hits, axis=2)
    weight = jnp.sum(jnp.where(hits, route_weight[None], 0.0), axis=2)
    order = jnp.arange(tok_rows, dtype=jnp.int32)
    before = (order[:, None] < order[None, :]).astype(jnp.bfloat16)
    rank = jnp.dot(chosen.astype(jnp.bfloat16), before, preferred_element_type=jnp.float32)
    rank = jnp.where(chosen, rank.astype(jnp.int32), -1)
    slots = jnp.arange(capacity, dtype=jnp.int32)
    placed = rank[:, None, :] == slots[None, :, None]
    return placed.astype(jnp.bfloat16), weight


def per_device(
    cotangent, moe_input, routes, route_weight, conv_input, input_gate, output_gate, conv_output,
    taps, w_out, w_gate, w_up, w_down,
):
    experts = lax.axis_size("sp")
    tp_size = lax.axis_size("tp")
    tok_rows, top_k = routes.shape
    capacity = -(-max(2, 2 * tok_rows * top_k // experts) // 16) * 16
    placed, weight = slot_masks(routes, route_weight, experts, capacity)
    returned, mixed_all, gate_wgrad, up_wgrad, grad_down = expert_exchange(
        experts, tp_size, capacity, moe_input, cotangent, placed, weight, output_gate, conv_output,
        w_gate[0], w_up[0], w_down[0],
    )
    grad_w_out, grad_mixed, grad_conv = mixer(
        experts, tp_size, placed, cotangent, output_gate, returned, mixed_all, w_out
    )
    (
        grad_output_gate, grad_conv_input, grad_input_gate, gate_wgrad, up_wgrad, grad_down, grad_w_out
    ) = finish(
        grad_mixed, grad_conv, conv_output, input_gate, conv_input, taps,
        gate_wgrad, up_wgrad, grad_down, grad_w_out,
    )
    return (
        gate_wgrad[None], up_wgrad[None], grad_down[None], grad_w_out,
        grad_conv_input, grad_input_gate, grad_output_gate,
    )


def solution(mesh):
    return jax.shard_map(
        per_device,
        mesh=mesh,
        in_specs=(
            P("sp", None), P("sp", None), P("sp", None), P("sp", None),
            P("sp", "tp"), P("sp", "tp"), P("sp", "tp"), P("sp", "tp"),
            P(None, "tp"), P(None, "tp"),
            P("sp", None, "tp"), P("sp", None, "tp"), P("sp", "tp", None),
        ),
        out_specs=(
            P("sp", None, "tp"), P("sp", None, "tp"), P("sp", "tp", None),
            P("sp", "tp"), P("sp", "tp"), P("sp", "tp"), P("sp", "tp"),
        ),
        check_vma=False,
    )
```

```python
import functools

import jax
import jax.numpy as jnp
from jax import lax
from jax.experimental import pallas as pl
from jax.experimental.pallas import tpu as pltpu
from jax.sharding import PartitionSpec as P

NEAR = 4
CUTS = 4
MESH = pl.DeviceIdType.MESH
NN = (((1,), (0,)), ((), ()))
NT = (((1,), (1,)), ((), ()))
TN = (((0,), (0,)), ((), ()))


def dot(a, b, dims=NN):
    return lax.dot_general(a, b, dims, preferred_element_type=jnp.float32)


def each(low, high, step):
    def body(i, carry):
        step(i)
        return carry

    lax.fori_loop(low, high, body, 0)


def spot():
    s, t = lax.axis_index("sp"), lax.axis_index("tp")
    return s, t, lax.div(t, 2), lax.rem(t, 2)


def flip(S, a, b):
    total, weight = 0, 1
    while weight < S:
        p, q = lax.rem(lax.div(a, weight), 2), lax.rem(lax.div(b, weight), 2)
        total, weight = total + (p + q - 2 * p * q) * weight, 2 * weight
    return total


def partner(S, s, i):
    if S < 4:
        return i
    high, low = lax.div(s, S // 2), lax.rem(lax.div(s, S // 4), 2)
    inner = high + low - 2 * high * low
    turned = S // 2 + lax.rem(i - S // 2 + inner * (S // 4) + S, S // 2)
    return jnp.where(i >= S // 2, turned, i)


def remote(src, dst, send, recv, device):
    return pltpu.make_async_remote_copy(
        src_ref=src, dst_ref=dst, send_sem=send, recv_sem=recv, device_id=device, device_id_type=MESH
    )


def greet(S, TH):
    s, t, th, tl = spot()
    barrier = pltpu.get_barrier_semaphore()

    def hello(device):
        pl.semaphore_signal(barrier, inc=1, device_id=device, device_id_type=MESH)

    each(1, S, lambda k: hello((lax.rem(s + k, S), t)))
    hello((s, 2 * th + 1 - tl))
    for j in range(1, TH):
        hello((s, 2 * lax.rem(th + j, TH) + tl))
    pl.semaphore_wait(barrier, S - 1 + TH)


def expert_kernel(
    S, T, inp, cot, placed, weight, out_gate, conv_out, wg_h, wu_h, wd_h,
    back, mix_all, gwg_h, gwu_h, gwd_h,
    mix, rows, stage, wgu, wd, proj, hid, ggu, part, matebuf, total_part, near, xsend, xrecv, rstage, gout, gdown,
    wsem, gsem, ds, dr, m1s, m1r, xs, xr, m2s, m2r, r1s, r1r, r2s, r2r, rts, rtr, us, ur, vs, vr, ys, yr,
):
    TH = T // 2
    cap, Q = rows.shape[3], rows.shape[4]
    D = T * Q
    H = wd.shape[0]
    piece = Q // S
    group = D // S
    s, t, th, tl = spot()
    mate = 2 * th + 1 - tl
    source = (inp, cot)

    def other(j):
        return lax.rem(th + j, TH)

    def behind(j):
        return lax.rem(th - j + TH, TH)

    def src_of(k):
        return flip(S, s, k)

    def at(i):
        return partner(S, s, i)

    weights = [
        pltpu.make_async_copy(wg_h, wgu.at[:, pl.ds(0, H)], wsem.at[0]),
        pltpu.make_async_copy(wu_h, wgu.at[:, pl.ds(H, H)], wsem.at[1]),
        pltpu.make_async_copy(wd_h, wd, wsem.at[2]),
    ]
    for copy in weights:
        copy.start()
    greet(S, TH)

    def direct(a, k):
        return remote(stage.at[a, k], rows.at[a, s, t], ds.at[a, k], dr.at[a, k], (src_of(k), t))

    def direct_too(a, j, k):
        q = 2 * other(j) + tl
        return remote(near.at[a, j, k], rows.at[a, s, q], xs.at[a, j, k], xr.at[a, TH - j, k], (src_of(k), t))

    def to_mate(a, k):
        block = rows.at[a, src_of(k), t]
        return remote(block, block, m1s.at[a, k], m1r.at[a, k], (s, mate))

    def across(a, j, k):
        block = rows.at[a, src_of(k), t]
        return remote(block, block, xs.at[a, j, k], xr.at[a, j, k], (s, 2 * other(j) + tl))

    def on_to_mate(a, j, k):
        block = rows.at[a, src_of(k), 2 * behind(j) + tl]
        return remote(block, block, m2s.at[a, j, k], m2r.at[a, j, k], (s, mate))

    def pick(a, e, columns):
        picked = dot(placed[e], source[a][:, columns])
        if a == 1:
            picked = picked * jnp.sum(placed[e].astype(jnp.float32) * weight[pl.ds(e, 1), :], axis=1, keepdims=True)
        return picked.astype(jnp.bfloat16)

    def send(a, k):
        stage[a, k] = pick(a, src_of(k), pl.ds(pl.multiple_of(t * Q, Q), Q))
        direct(a, k).start()

        @pl.when(k < NEAR)
        def _():
            for j in range(1, TH):
                near[a, j, k] = pick(a, src_of(k), pl.ds(pl.multiple_of((2 * other(j) + tl) * Q, Q), Q))
                direct_too(a, j, k).start()

    def own(a):
        for q in range(T):
            rows[a, s, q] = pick(a, s, pl.ds(q * Q, Q))

    def forward(a, k):
        direct(a, k).wait_recv()

        @pl.when(k >= NEAR)
        def _():
            for j in range(1, TH):
                across(a, j, k).start()

        to_mate(a, k).start()

    def forward_on(a, k):
        for j in range(1, TH):
            across(a, j, k).wait_recv()
            on_to_mate(a, j, k).start()

    def complete(a, k):
        to_mate(a, k).wait_recv()
        for j in range(1, TH):
            on_to_mate(a, j, k).wait_recv()

    def project(k):
        b = src_of(k)
        total = dot(rows[0, b, 0], wgu[pl.ds(0, Q), :])
        for q in range(1, T):
            total = total + dot(rows[0, b, q], wgu[pl.ds(q * Q, Q), :])
        proj[b] = total

    def half(n):
        return remote(part.at[lax.rem(n, 2), 1 - tl], matebuf.at[n], r1s.at[n], r1r.at[n], (s, mate))

    def chip_sum(j, k):
        return remote(xsend.at[j, k], xrecv.at[j, k], r2s.at[j, k], r2r.at[j, k], (s, 2 * other(j) + tl))

    def give_back(k):
        return remote(rstage.at[k], back.at[s], rts.at[k], rtr.at[k], (src_of(k), t))

    def gradients(n, k):
        b = src_of(k)
        grad_hidden = dot(rows[1, b, 0], wd[:, pl.ds(0, Q)], NT)
        for q in range(1, T):
            grad_hidden = grad_hidden + dot(rows[1, b, q], wd[:, pl.ds(q * Q, Q)], NT)
        gate, up = proj[b][:, :H], proj[b][:, H:]
        sig = jax.nn.sigmoid(gate)
        act = gate * sig
        slope = sig * (1.0 + gate * (1.0 - sig))
        hid[b] = (act * up).astype(jnp.bfloat16)
        ggu[b, :, pl.ds(0, H)] = (grad_hidden * up * slope).astype(jnp.bfloat16)
        ggu[b, :, pl.ds(H, H)] = (grad_hidden * act).astype(jnp.bfloat16)

        @pl.when(n >= 2)
        def _():
            half(n - 2).wait_send()

        slot = lax.rem(n, 2)
        grads = ggu[b]
        for g in range(S):
            some = dot(grads, wgu[pl.ds(g * group, group), :], NT)
            for q in range(T):
                part[slot, q % 2, q // 2, :, pl.ds(g * piece, piece)] = some[:, q * piece : (q + 1) * piece]
        half(n).start()

    def reduce_chip(n, k):
        half(n).wait_recv()
        slot = lax.rem(n, 2)
        for j in range(1, TH):
            o = other(j)
            xsend[j, k] = (part[slot, tl, o] + matebuf[n, o]).astype(jnp.bfloat16)
            chip_sum(j, k).start()
        total_part[lax.rem(n, 3)] = part[slot, tl, th] + matebuf[n, th]

    def reduce_all(n, k):
        total = total_part[lax.rem(n, 3)]
        for j in range(1, TH):
            chip_sum(j, k).wait_recv()
            total = total + xrecv[j, k].astype(jnp.float32)
        rstage[k] = total.astype(jnp.bfloat16)

        @pl.when(k >= 1)
        def _():
            give_back(k).start()

    SH = S // 2
    sh, sl = lax.div(s, 2), lax.rem(s, 2)

    def block(h):
        return mix_all.at[2 * h + sl]

    def rise(j):
        return remote(mix if j == 0 else block(sh - j), block(sh - j), us.at[j], ur.at[j + 1], (s + 2, t))

    def sink(j):
        return remote(mix if j == 0 else block(sh + j), block(sh + j), vs.at[j], vr.at[j + 1], (s - 2, t))

    def side(h, value=None):
        return remote(block(h) if value is None else value, block(h), ys.at[h], yr.at[h], (2 * sh + 1 - sl, t))

    def mix_step(j):
        if j == 0:
            side(sh, mix).start()

            @pl.when(sh < SH - 1)
            def _():
                rise(0).start()

            @pl.when(sh > 0)
            def _():
                sink(0).start()

            return

        @pl.when(sh >= j)
        def _():
            remote(block(sh - j), block(sh - j), us.at[j], ur.at[j], (s, mate)).wait_recv()

            @pl.when(sh < SH - 1)
            def _():
                rise(j).start()

            side(sh - j).start()

        @pl.when(sh + j < SH)
        def _():
            remote(block(sh + j), block(sh + j), vs.at[j], vr.at[j], (s, mate)).wait_recv()

            @pl.when(sh > 0)
            def _():
                sink(j).start()

            side(sh + j).start()

    def mix_finish():
        keep_mix.wait()
        for j in range(SH - 1):

            @pl.when((sh >= j) & (sh < SH - 1))
            def _():
                rise(j).wait_send()

            @pl.when((sh + j < SH) & (sh > 0))
            def _():
                sink(j).wait_send()

        def one(h):
            side(h).wait_send()
            side(h).wait_recv()

        each(0, SH, one)

    keep_mix = pltpu.make_async_copy(mix, mix_all.at[s], gsem.at[3])
    keep = pltpu.make_async_copy(rstage.at[0], back.at[s], rts.at[0])

    mix[...] = (out_gate[...].astype(jnp.float32) * conv_out[...].astype(jnp.float32)).astype(jnp.bfloat16)
    middle = max(2, S // 2)
    each(middle, S, lambda i: send(0, at(i)))
    mix_step(0)
    each(1, middle, lambda i: send(0, at(i)))
    each(1, middle, lambda i: send(1, at(i)))
    own(0)
    own(1)
    for copy in weights:
        copy.wait()
    project(0)
    gradients(0, 0)

    def first(i):
        @pl.when(i < S)
        def _():
            forward(0, at(i))

        @pl.when(i == S - 1)
        def _():
            each(middle, S, lambda m: send(1, at(m)))

        @pl.when(i == middle + 1)
        def _():
            reduce_chip(0, 0)

        @pl.when(i == middle + 3)
        def _():
            reduce_all(0, 0)

        @pl.when((i >= middle + 1) & (i < S + 1))
        def _():
            forward_on(0, at(i - 1))

        @pl.when(i >= middle + 2)
        def _():
            complete(0, at(i - 2))
            project(at(i - 2))

    each(middle, S + 2, first)
    mix_step(1)

    lead = S // 4

    def near_at(i):
        return (i > lead) & (i < lead + middle)

    def then(i):
        return jnp.where(i <= lead, at(i + middle - 1), jnp.where(i < lead + middle, at(i - lead), at(i)))

    def second(i):
        @pl.when(near_at(i))
        def _():
            forward(0, then(i))

        @pl.when(i < S)
        def _():
            forward(1, then(i))

        @pl.when((i >= 4) & (i < S + 3))
        def _():
            reduce_chip(i - 3, then(i - 3))

        @pl.when(near_at(i - 1))
        def _():
            forward_on(0, then(i - 1))

        @pl.when((i >= 2) & (i < S + 1))
        def _():
            forward_on(1, then(i - 1))

        @pl.when(near_at(i - 2))
        def _():
            complete(0, then(i - 2))
            project(then(i - 2))

        @pl.when((i >= 3) & (i < S + 2))
        def _():
            complete(1, then(i - 2))
            gradients(i - 2, then(i - 2))

        @pl.when(i >= 6)
        def _():
            reduce_all(i - 5, then(i - 5))

        for j in range(2, SH):

            @pl.when(i == S // 2 + 1 + (S // 2) * (j - 1) // (SH - 1))
            def _():
                mix_step(j)

    each(1, S + 5, second)
    keep.start()
    keep_mix.start()

    tile = min(512, Q)
    per = Q // tile

    def weight_grads(i):
        q, c = lax.div(i, per), pl.multiple_of(lax.rem(i, per) * tile, tile)
        x = rows[0, :, q, :, pl.ds(c, tile)].reshape(S * cap, tile)
        start = pl.multiple_of(q * Q + c, tile)
        gout[pl.ds(start, tile), :] = dot(x, ggu[...].reshape(S * cap, 2 * H), TN).astype(jnp.bfloat16)
        d = rows[1, :, q, :, pl.ds(c, tile)].reshape(S * cap, tile)
        gdown[:, pl.ds(start, tile)] = dot(hid[...].reshape(S * cap, H), d, TN).astype(jnp.bfloat16)

    each(0, T * per, weight_grads)
    results = [
        pltpu.make_async_copy(gout.at[:, pl.ds(0, H)], gwg_h, gsem.at[0]),
        pltpu.make_async_copy(gout.at[:, pl.ds(H, H)], gwu_h, gsem.at[1]),
        pltpu.make_async_copy(gdown, gwd_h, gsem.at[2]),
    ]
    for copy in results:
        copy.start()

    half(S - 2).wait_send()
    half(S - 1).wait_send()

    def finish(k):
        for a in range(2):
            direct(a, k).wait_send()
            to_mate(a, k).wait_send()
            for j in range(1, TH):
                across(a, j, k).wait_send()
                on_to_mate(a, j, k).wait_send()
        give_back(k).wait_send()
        give_back(k).wait_recv()

    each(1, S, finish)

    def finish_sums(k):
        for j in range(1, TH):
            chip_sum(j, k).wait_send()

    each(0, S, finish_sums)
    keep.wait()
    mix_finish()
    for copy in results:
        copy.wait()


def mixer_kernel(
    S, T, placed, cot, out_gate, back_h, mix_h, w_out_h,
    gwo, gm, shifted,
    back, mix, w_out, total, res, colst, near, cols, conv, after,
    lsem, ds, dr, m1s, m1r, xs, xr, m2s, m2r, bs, br,
):
    TH = T // 2
    cap, Q = back.shape[1], back.shape[2]
    tok = cot.shape[0]
    piece, group = Q // S, T * Q // S
    s, t, th, tl = spot()
    mate = 2 * th + 1 - tl
    local = [
        pltpu.make_async_copy(src, dst, lsem.at[n])
        for n, (src, dst) in enumerate(((back_h, back), (mix_h, mix), (w_out_h, w_out)))
    ]
    for copy in local:
        copy.start()
    greet(S, TH)

    def other(j):
        return lax.rem(th + j, TH)

    def behind(j):
        return lax.rem(th - j + TH, TH)

    def at(i):
        return partner(S, s, i)

    def direct(k):
        peer = flip(S, s, k)
        return remote(colst.at[peer], cols.at[s, t], ds.at[k], dr.at[k], (peer, t))

    def direct_too(j, k):
        peer = flip(S, s, k)
        land = cols.at[s, 2 * other(j) + tl]
        return remote(near.at[j, k], land, xs.at[j, k], xr.at[TH - j, k], (peer, t))

    def block(k, q):
        return cols.at[flip(S, s, k), q] if k is not None else res.at[q]

    def to_mate(k):
        n = S if k is None else k
        return remote(block(k, t), block(k, t), m1s.at[n], m1r.at[n], (s, mate))

    def across(j, k):
        n = S if k is None else k
        return remote(block(k, t), block(k, t), xs.at[j, n], xr.at[j, n], (s, 2 * other(j) + tl))

    def on_to_mate(j, k):
        n = S if k is None else k
        q = 2 * behind(j) + tl
        return remote(block(k, q), block(k, q), m2s.at[j, n], m2r.at[j, n], (s, mate))

    def forward(k):
        @pl.when((S if k is None else k) >= NEAR)
        def _():
            for j in range(1, TH):
                across(j, k).start()

        to_mate(k).start()

    def forward_on(k):
        for j in range(1, TH):
            across(j, k).wait_recv()
            on_to_mate(j, k).start()

    def complete(k):
        to_mate(k).wait_recv()
        for j in range(1, TH):
            on_to_mate(j, k).wait_recv()

    def sent(k):
        to_mate(k).wait_send()
        for j in range(1, TH):
            across(j, k).wait_send()
            on_to_mate(j, k).wait_send()

    local[0].wait()
    total[...] = dot(placed[...].reshape(S * cap, tok), back[...].reshape(S * cap, Q), TN)
    for q in range(T):

        @pl.when(t == q)
        def _():
            for g in range(S):
                columns = pl.ds(g * piece, piece)
                mine = cot[:, pl.ds(g * group + q * piece, piece)].astype(jnp.float32)
                value = (mine + total[:, columns]).astype(jnp.bfloat16)
                res[q, :, columns] = value
                colst[g] = value

    forward(None)
    each(1, S, lambda i: direct(at(i)).start())

    def arrive(i):
        direct(at(i)).wait_recv()
        forward(at(i))

    local[2].wait()
    forward_on(None)
    each(1, S, arrive)
    complete(None)
    for g in range(S):

        @pl.when(s == g)
        def _():
            for q in range(T):
                cols[s, q] = res[q, :, pl.ds(g * piece, piece)]

        for k in range(1, min(NEAR, S)):

            @pl.when(flip(S, s, k) == g)
            def _():
                for j in range(1, TH):
                    near[j, k] = res[2 * other(j) + tl, :, pl.ds(g * piece, piece)]
                    direct_too(j, k).start()

    grad_mixed = jnp.zeros((tok, w_out.shape[1]), jnp.float32)
    for g in range(S):
        some = jnp.concatenate([res[q, :, pl.ds(g * piece, piece)] for q in range(T)], axis=1)
        grad_mixed = grad_mixed + dot(some, w_out[pl.ds(g * group, group), :])
    gm[...] = grad_mixed
    conv[pl.ds(0, tok), :] = grad_mixed * out_gate[...].astype(jnp.float32)

    def edge(target):
        return remote(conv.at[pl.ds(0, 8), :], after, bs.at[0], br.at[0], (target, t))

    @pl.when(s > 0)
    def _():
        edge(s - 1).start()

    local[1].wait()

    def take(k):
        @pl.when(k > 0)
        def _():
            complete(k)
        b = flip(S, s, k)
        columns = jnp.concatenate([cols[b, q] for q in range(T)], axis=1)
        gwo[...] += dot(columns, mix[b], TN)

    gwo[...] = jnp.zeros_like(gwo)
    take(0)

    def turn(i):
        return at(jnp.where(i <= S - NEAR, i + NEAR - 1, i - (S - NEAR)))

    def step(i):
        @pl.when(i < S)
        def _():
            forward_on(turn(i))

        @pl.when(i >= 2)
        def _():
            take(turn(i - 1))

    each(1, S + 1, step)

    @pl.when(s < S - 1)
    def _():
        edge(0).wait_recv()
        conv[pl.ds(tok, 8), :] = after[...]

    @pl.when(s == S - 1)
    def _():
        conv[pl.ds(tok, 8), :] = jnp.zeros_like(after)

    shifted[...] = conv[...]

    @pl.when(s > 0)
    def _():
        edge(s - 1).wait_send()

    sent(None)
    each(1, S, sent)
    each(1, S, lambda k: direct(k).wait_send())


def expert_exchange(S, T, cap, inp, cot, placed, weight, out_gate, conv_out, w_gate, w_up, w_down):
    tok, D = inp.shape
    H = w_down.shape[0]
    TH, Q, SH = T // 2, D // T, S // 2
    bf, f32 = jnp.bfloat16, jnp.float32
    dma = pltpu.SemaphoreType.DMA
    vmem = pl.BlockSpec(memory_space=pltpu.VMEM)
    hbm = pl.BlockSpec(memory_space=pl.ANY)
    rows = S * cap
    return pl.pallas_call(
        functools.partial(expert_kernel, S, T),
        name="expert_exchange",
        out_shape=(
            jax.ShapeDtypeStruct((S, cap, Q), bf),
            jax.ShapeDtypeStruct((S,) + out_gate.shape, bf),
            jax.ShapeDtypeStruct((D, H), bf),
            jax.ShapeDtypeStruct((D, H), bf),
            jax.ShapeDtypeStruct((H, D), bf),
        ),
        in_specs=[vmem] * 6 + [hbm] * 3,
        out_specs=(hbm,) * 5,
        scratch_shapes=[
            pltpu.VMEM(out_gate.shape, bf),
            pltpu.VMEM((2, S, T, cap, Q), bf),
            pltpu.VMEM((2, S, cap, Q), bf),
            pltpu.VMEM((D, 2 * H), bf),
            pltpu.VMEM((H, D), bf),
            pltpu.VMEM((S, cap, 2 * H), f32),
            pltpu.VMEM((S, cap, H), bf),
            pltpu.VMEM((S, cap, 2 * H), bf),
            pltpu.VMEM((2, 2, TH, cap, Q), f32),
            pltpu.VMEM((S, TH, cap, Q), f32),
            pltpu.VMEM((3, cap, Q), f32),
            pltpu.VMEM((2, TH, NEAR, cap, Q), bf),
            pltpu.VMEM((TH, S, cap, Q), bf),
            pltpu.VMEM((TH, S, cap, Q), bf),
            pltpu.VMEM((S, cap, Q), bf),
            pltpu.VMEM((D, 2 * H), bf),
            pltpu.VMEM((H, D), bf),
            dma((3,)), dma((4,)),
            dma((2, S)), dma((2, S)),
            dma((2, S)), dma((2, S)),
            dma((2, TH, S)), dma((2, TH, S)),
            dma((2, TH, S)), dma((2, TH, S)),
            dma((S,)), dma((S,)),
            dma((TH, S)), dma((TH, S)),
            dma((S,)), dma((S,)),
            dma((SH,)), dma((SH + 1,)),
            dma((SH,)), dma((SH + 1,)),
            dma((SH,)), dma((SH,)),
        ],
        cost_estimate=pl.CostEstimate(
            flops=16 * rows * D * H, bytes_accessed=8 * rows * D + 24 * D * H, transcendentals=rows * H
        ),
        compiler_params=pltpu.CompilerParams(
            collective_id=0, has_side_effects=True, vmem_limit_bytes=67_043_328
        ),
    )(inp, cot, placed, weight, out_gate, conv_out, w_gate, w_up, w_down)


def mixer(S, T, placed, cot, out_gate, back, mix_all, w_out):
    tok, D = cot.shape
    B = w_out.shape[1]
    cap = placed.shape[1]
    TH, Q = T // 2, D // T
    bf, f32 = jnp.bfloat16, jnp.float32
    dma = pltpu.SemaphoreType.DMA
    vmem = pl.BlockSpec(memory_space=pltpu.VMEM)
    hbm = pl.BlockSpec(memory_space=pl.ANY)
    return pl.pallas_call(
        functools.partial(mixer_kernel, S, T),
        name="mixer",
        out_shape=tuple(jax.ShapeDtypeStruct((n, B), f32) for n in (D // S, tok, tok + 8)),
        in_specs=[vmem] * 3 + [hbm] * 3,
        out_specs=(vmem,) * 3,
        scratch_shapes=[
            pltpu.VMEM((S, cap, Q), bf),
            pltpu.VMEM((S, tok, B), bf),
            pltpu.VMEM((D, B), bf),
            pltpu.VMEM((tok, Q), f32),
            pltpu.VMEM((T, tok, Q), bf),
            pltpu.VMEM((S, tok, Q // S), bf),
            pltpu.VMEM((TH, NEAR, tok, Q // S), bf),
            pltpu.VMEM((S, T, tok, Q // S), bf),
            pltpu.VMEM((tok + 8, B), f32),
            pltpu.VMEM((8, B), f32),
            dma((3,)),
            dma((S,)), dma((S,)),
            dma((S + 1,)), dma((S + 1,)),
            dma((TH, S + 1)), dma((TH, S + 1)),
            dma((TH, S + 1)), dma((TH, S + 1)),
            dma((1,)), dma((1,)),
        ],
        cost_estimate=pl.CostEstimate(
            flops=2 * tok * D * B * 2 + 2 * S * cap * tok * Q, bytes_accessed=4 * D * B, transcendentals=0
        ),
        compiler_params=pltpu.CompilerParams(
            collective_id=1, has_side_effects=True, vmem_limit_bytes=67_043_328
        ),
    )(placed, cot, out_gate, back, mix_all, w_out)


def finish_kernel(parts, gm, conv, conv_out, in_gate, conv_in, taps, *refs):
    n = len(parts)
    ins, gog, gci, gig, outs = refs[:n], refs[n], refs[n + 1], refs[n + 2], refs[n + 3 : 2 * n + 3]
    held, insem, outsem = refs[2 * n + 3 : 3 * n + 3], refs[3 * n + 3], refs[3 * n + 4]
    tok = gm.shape[0]
    pieces = []
    for m in range(n):
        rows = parts[m].shape[0] // CUTS
        for c in range(CUTS):
            cut, sem = pl.ds(c * rows, rows), m * CUTS + c
            take = pltpu.make_async_copy(ins[m].at[cut, :], held[m].at[cut, :], insem.at[sem])
            give = pltpu.make_async_copy(held[m].at[cut, :], outs[m].at[cut, :], outsem.at[sem])
            take.start()
            pieces.append((take, give))
    for take, give in pieces[: len(pieces) // 2]:
        take.wait()
        give.start()
    grad_g = (
        taps[2:3, :] * conv[pl.ds(0, tok), :]
        + taps[1:2, :] * conv[pl.ds(1, tok), :]
        + taps[0:1, :] * conv[pl.ds(2, tok), :]
    )
    gog[...] = (gm[...] * conv_out[...].astype(jnp.float32)).astype(jnp.bfloat16)
    gci[...] = (grad_g * in_gate[...].astype(jnp.float32)).astype(jnp.bfloat16)
    gig[...] = (grad_g * conv_in[...].astype(jnp.float32)).astype(jnp.bfloat16)
    for take, give in pieces[len(pieces) // 2 :]:
        take.wait()
        give.start()
    for _, give in pieces:
        give.wait()


def finish(gm, conv, conv_out, in_gate, conv_in, taps, *parts):
    vmem = pl.BlockSpec(memory_space=pltpu.VMEM)
    hbm = pl.BlockSpec(memory_space=pl.ANY)
    shapes = tuple(jax.ShapeDtypeStruct(part.shape, part.dtype) for part in parts)
    small = jax.ShapeDtypeStruct(conv_out.shape, conv_out.dtype)
    return pl.pallas_call(
        functools.partial(finish_kernel, shapes),
        name="finish",
        out_shape=(small, small, small) + shapes,
        in_specs=[vmem] * 6 + [hbm] * len(parts),
        out_specs=(vmem,) * 3 + (hbm,) * len(parts),
        scratch_shapes=[pltpu.VMEM(part.shape, part.dtype) for part in parts]
        + [pltpu.SemaphoreType.DMA((len(parts) * CUTS,))] * 2,
        compiler_params=pltpu.CompilerParams(vmem_limit_bytes=67_043_328),
    )(gm, conv, conv_out, in_gate, conv_in, taps, *parts)


def slot_masks(routes, route_weight, experts, capacity):
    tok_rows = routes.shape[0]
    names = jnp.arange(experts, dtype=jnp.int32)
    hits = routes[None, :, :] == names[:, None, None]
    chosen = jnp.any(hits, axis=2)
    weight = jnp.sum(jnp.where(hits, route_weight[None], 0.0), axis=2)
    order = jnp.arange(tok_rows, dtype=jnp.int32)
    before = (order[:, None] < order[None, :]).astype(jnp.bfloat16)
    rank = jnp.dot(chosen.astype(jnp.bfloat16), before, preferred_element_type=jnp.float32)
    rank = jnp.where(chosen, rank.astype(jnp.int32), -1)
    slots = jnp.arange(capacity, dtype=jnp.int32)
    placed = rank[:, None, :] == slots[None, :, None]
    return placed.astype(jnp.bfloat16), weight


def per_device(
    cotangent, moe_input, routes, route_weight, conv_input, input_gate, output_gate, conv_output,
    taps, w_out, w_gate, w_up, w_down,
):
    experts = lax.axis_size("sp")
    tp_size = lax.axis_size("tp")
    tok_rows, top_k = routes.shape
    capacity = -(-max(2, 2 * tok_rows * top_k // experts) // 16) * 16
    placed, weight = slot_masks(routes, route_weight, experts, capacity)
    returned, mixed_all, gate_wgrad, up_wgrad, grad_down = expert_exchange(
        experts, tp_size, capacity, moe_input, cotangent, placed, weight, output_gate, conv_output,
        w_gate[0], w_up[0], w_down[0],
    )
    grad_w_out, grad_mixed, grad_conv = mixer(
        experts, tp_size, placed, cotangent, output_gate, returned, mixed_all, w_out
    )
    (
        grad_output_gate, grad_conv_input, grad_input_gate, gate_wgrad, up_wgrad, grad_down, grad_w_out
    ) = finish(
        grad_mixed, grad_conv, conv_output, input_gate, conv_input, taps,
        gate_wgrad, up_wgrad, grad_down, grad_w_out,
    )
    return (
        gate_wgrad[None], up_wgrad[None], grad_down[None], grad_w_out,
        grad_conv_input, grad_input_gate, grad_output_gate,
    )


def solution(mesh):
    return jax.shard_map(
        per_device,
        mesh=mesh,
        in_specs=(
            P("sp", None), P("sp", None), P("sp", None), P("sp", None),
            P("sp", "tp"), P("sp", "tp"), P("sp", "tp"), P("sp", "tp"),
            P(None, "tp"), P(None, "tp"),
            P("sp", None, "tp"), P("sp", None, "tp"), P("sp", "tp", None),
        ),
        out_specs=(
            P("sp", None, "tp"), P("sp", None, "tp"), P("sp", "tp", None),
            P("sp", "tp"), P("sp", "tp"), P("sp", "tp"), P("sp", "tp"),
        ),
        check_vma=False,
    )
```
